128 devices in a mesh: sp: 16 (over z, x), tp: 8 (over y, core).
Axes of the slice: x: 4, y: 4, z: 4, core: 2. Of those that a mesh axis runs over, the one named last changes fastest.
Arguments:
- tokens: bfloat16 [4, 16384, 2048], P(None, 'sp'), may hold values from -6 to 6
- norm_gain: bfloat16 [2048], replicated, may hold values from 0.099609375 to 1.8984375
- conv_value_weight: bfloat16 [2048, 1024], P('sp', 'tp'), may hold values from -0.125 to 0.125
- conv_gate_weight: bfloat16 [2048, 1024], P('sp', 'tp'), may hold values from -0.125 to 0.125
- query_weight: bfloat16 [2048, 1024], P('sp', 'tp'), may hold values from -40 to 40
- key_weight: bfloat16 [2048, 512], P('sp', 'tp'), may hold values from -1 to 1
- value_weight: bfloat16 [2048, 512], P('sp', 'tp'), may hold values from -0.125 to 0.125
- conv_taps: bfloat16 [31, 1024], P(None, 'tp'), may hold values from -1 to 1
- conv_gain: bfloat16 [1024], P('tp'), may hold values from 0.099609375 to 1.8984375
- sink_logit: float32 [16], P('tp'), may hold values from 1 to 6
- out_conv_weight: bfloat16 [1024, 2048], P('tp', 'sp'), may hold values from -0.125 to 0.125
- out_attn_weight: bfloat16 [1024, 2048], P('tp', 'sp'), may hold values from -0.125 to 0.125
Outputs:
- mixed: bfloat16 [4, 16384, 2048], P(None, ('sp', 'tp'))
- log_total: float32 [4, 16, 16384], P(None, 'tp', 'sp')
The draws below stay inside these ranges and needn't reach their ends.
All inputs are finite; a program needn't handle non-finite values.
Results may differ from the reference program's by a relative error of at most 0.015.
Values may be sent and summed in bfloat16 or wider, within the bound.
A program may use at most 128 MiB of HBM per device.

```python
import math
import jax
import jax.numpy as jnp
from jax import lax

D = 2048
CONV_CH = 1024
HEADS = 16
KV_HEADS = 8
HEAD_DIM = 64
WINDOW = 128
CONV_K = 31
SEQS = 4
SEQ = 16384


def shared_keys(key):
    drawn = jax.random.truncated_normal(jax.random.fold_in(key, 71), -6.0, 6.0, (D, KV_HEADS * HEAD_DIM), jnp.float32)
    return drawn / jnp.sqrt(jnp.float32(D))


def draw_key_weight(key, part):
    return shared_keys(key).astype(jnp.bfloat16)


def draw_query_weight(key, part):
    drawn = jax.random.truncated_normal(jax.random.fold_in(key, 73), -6.0, 6.0, (D, HEADS * HEAD_DIM), jnp.float32)
    drawn = drawn / jnp.sqrt(jnp.float32(D))
    return drawn.astype(jnp.bfloat16)


def levels(stream_key, shape, split, smallest, largest):
    def one(dim, shards_of):
        heights = jax.random.uniform(jax.random.fold_in(jax.random.fold_in(stream_key, 6), dim), (shards_of,), jnp.float32, smallest / len(split), largest / len(split))
        return jnp.repeat(jnp.exp(heights), shape[dim] // shards_of).reshape((-1,) + (1,) * (len(shape) - dim - 1))

    gain = one(*split[0])
    for cut in split[1:]:
        gain = gain * one(*cut)
    return gain


def noise(key, dims, deviation, limit, pieces=(), kind=jnp.bfloat16):
    loudness = levels(key, dims, pieces, -0.22, 0.18) if pieces else 1.0
    result = jax.random.normal(key, dims, jnp.float32) * deviation * loudness
    return jnp.minimum(jnp.maximum(result, -limit), limit).astype(kind)


def setup_inputs(seed: int = 0) -> dict:
    streams_of = jax.random.split(jax.random.key(seed), 13)
    tokens = noise(streams_of[0], (SEQS, SEQ, D), 1.0, 6.0, ((1, 16),))
    norm_gain = jnp.clip(1.0 + 0.18 * jax.random.normal(streams_of[1], (D,), jnp.float32), 0.099609375, 1.8984375).astype(jnp.bfloat16)
    conv_value_weight = noise(streams_of[2], (D, CONV_CH), D ** -0.5, 0.125, ((0, 16), (1, 8)))
    conv_gate_weight = noise(streams_of[3], (D, CONV_CH), D ** -0.5, 0.125, ((0, 16), (1, 8)))
    query_weight = draw_query_weight(jax.random.fold_in(streams_of[12], 71), 0)
    key_weight = draw_key_weight(jax.random.fold_in(streams_of[12], 71), 0)
    value_weight = noise(streams_of[6], (D, KV_HEADS * HEAD_DIM), D ** -0.5, 0.125, ((0, 16), (1, 8)))
    conv_taps = noise(streams_of[7], (CONV_K, CONV_CH), CONV_K ** -0.5, 1.0, ((1, 8),))
    conv_gain = jnp.clip(1.0 + 0.18 * jax.random.normal(streams_of[8], (CONV_CH,), jnp.float32), 0.099609375, 1.8984375).astype(jnp.bfloat16)
    sink_logit = jnp.clip(1.0 + 5.0 * jax.random.uniform(streams_of[9], (HEADS,), jnp.float32) ** levels(streams_of[9], (HEADS,), ((0, 8),), -0.2, 0.2), 1.0, 6.0)
    out_conv_weight = noise(streams_of[10], (CONV_CH, D), (CONV_CH + HEADS * HEAD_DIM) ** -0.5, 0.125, ((0, 8), (1, 16)))
    out_attn_weight = noise(streams_of[11], (HEADS * HEAD_DIM, D), (CONV_CH + HEADS * HEAD_DIM) ** -0.5, 0.125, ((0, 8), (1, 16)))
    return dict(tokens=tokens, norm_gain=norm_gain, conv_value_weight=conv_value_weight, conv_gate_weight=conv_gate_weight, query_weight=query_weight, key_weight=key_weight, value_weight=value_weight, conv_taps=conv_taps, conv_gain=conv_gain, sink_logit=sink_logit, out_conv_weight=out_conv_weight, out_attn_weight=out_attn_weight)


EPSILON = 1e-06
ROPE_BASE = 10000.0
MASK_VALUE = -1e+30

def rotate(raw, positions):
    half_dim = raw.shape[-1] // 2
    inverse = ROPE_BASE ** (-jnp.arange(half_dim, dtype=jnp.float32) / half_dim)
    angles = positions[:, None] * inverse[None, :]
    cosine = jnp.cos(angles)[None, :, None, :]
    sine = jnp.sin(angles)[None, :, None, :]
    first, second = (raw[..., :half_dim], raw[..., half_dim:])
    return jnp.concatenate([first * cosine - second * sine, first * sine + second * cosine], axis=-1)

def reference(tokens, norm_gain, conv_value_weight, conv_gate_weight, query_weight, key_weight, value_weight, conv_taps, conv_gain, sink_logit, out_conv_weight, out_attn_weight):
    seq_count, seq_len, width = tokens.shape
    floats = tokens.astype(jnp.float32)
    row_mean = floats.mean(-1, keepdims=True)
    centred = floats - row_mean
    variance = lax.optimization_barrier(jnp.mean(centred * centred, -1, keepdims=True))
    normed = (centred * lax.rsqrt(variance + EPSILON) * norm_gain.astype(jnp.float32)).astype(jnp.bfloat16)
    flat = normed.reshape(-1, width)
    conv_value = jnp.dot(flat, conv_value_weight, preferred_element_type=jnp.float32)
    conv_gate = jnp.dot(flat, conv_gate_weight, preferred_element_type=jnp.float32)
    gated = (conv_value * jax.nn.sigmoid(conv_gate)).astype(jnp.bfloat16).reshape(seq_count, seq_len, CONV_CH)
    rim = CONV_K // 2
    padded = jnp.pad(gated, ((0, 0), (rim, rim), (0, 0)))
    taps = conv_taps.astype(jnp.float32)
    filtered = jnp.zeros((seq_count, seq_len, CONV_CH), jnp.float32)
    for tap_index in range(CONV_K):
        filtered = filtered + padded[:, tap_index:tap_index + seq_len].astype(jnp.float32) * taps[tap_index]
    chan_mean = filtered.mean(-1, keepdims=True)
    chan_centred = filtered - chan_mean
    chan_var = lax.optimization_barrier(jnp.mean(chan_centred * chan_centred, -1, keepdims=True))
    conv_out = jax.nn.silu(chan_centred * lax.rsqrt(chan_var + EPSILON) * conv_gain.astype(jnp.float32))
    conv_out = conv_out.astype(jnp.bfloat16)
    group = HEADS // KV_HEADS
    positions = jnp.arange(seq_len, dtype=jnp.float32)
    query_raw = jnp.dot(flat, query_weight, preferred_element_type=jnp.float32)
    key_raw = jnp.dot(flat, key_weight, preferred_element_type=jnp.float32)
    queries = rotate(query_raw.reshape(seq_count, seq_len, HEADS, HEAD_DIM), positions).astype(jnp.bfloat16)
    queries = queries.reshape(seq_count, seq_len, KV_HEADS, group, HEAD_DIM)
    keys = rotate(key_raw.reshape(seq_count, seq_len, KV_HEADS, HEAD_DIM), positions).astype(jnp.bfloat16)
    values = jnp.dot(flat, value_weight, preferred_element_type=jnp.float32).astype(jnp.bfloat16)
    values = values.reshape(seq_count, seq_len, KV_HEADS, HEAD_DIM)
    edge = ((0, 0), (WINDOW, WINDOW), (0, 0), (0, 0))
    keys_pad = jnp.pad(keys, edge)
    values_pad = jnp.pad(values, edge)
    block_rows = math.gcd(seq_len, 512)
    span_len = block_rows + 2 * WINDOW
    score_scale = HEAD_DIM ** (-0.5)
    sink = sink_logit.astype(jnp.float32).reshape(KV_HEADS, group)[None, :, :, None]
    relative = jnp.arange(span_len)[None, :] - jnp.arange(block_rows)[:, None]
    band = (relative >= 0) & (relative <= 2 * WINDOW)

    def one_block(block):
        first_row = (block * block_rows).astype(jnp.int32)
        q_block = lax.dynamic_slice_in_dim(queries, first_row, block_rows, 1).astype(jnp.float32)
        k_block = lax.dynamic_slice_in_dim(keys_pad, first_row, span_len, 1).astype(jnp.float32)
        v_block = lax.dynamic_slice_in_dim(values_pad, first_row, span_len, 1).astype(jnp.float32)
        scores = jnp.einsum('sqkgd,spkd->skgqp', q_block, k_block) * score_scale
        key_pos = first_row - WINDOW + jnp.arange(span_len, dtype=jnp.int32)
        allowed = band & ((key_pos >= 0) & (key_pos < seq_len))[None, :]
        scores = jnp.where(allowed, scores, MASK_VALUE)
        top = jnp.maximum(scores.max(-1), sink)
        weights = jnp.exp(scores - top[..., None])
        total = weights.sum(-1) + jnp.exp(sink - top)
        probs = (weights / total[..., None]).astype(jnp.bfloat16).astype(jnp.float32)
        out = jnp.einsum('skgqp,spkd->sqkgd', probs, v_block).astype(jnp.bfloat16)
        return (out, top + jnp.log(total))
    outs, totals = lax.map(one_block, jnp.arange(seq_len // block_rows, dtype=jnp.int32))
    attn_out = jnp.moveaxis(outs, 0, 1).reshape(seq_count * seq_len, HEADS * HEAD_DIM)
    log_total = jnp.moveaxis(totals, 0, 3).reshape(seq_count, HEADS, seq_len)
    mixed = jnp.dot(conv_out.reshape(-1, CONV_CH), out_conv_weight, preferred_element_type=jnp.float32) + jnp.dot(attn_out, out_attn_weight, preferred_element_type=jnp.float32)
    return (mixed.astype(jnp.bfloat16).reshape(seq_count, seq_len, width), log_total)
```

```python
import functools

import jax
import jax.numpy as jnp
from jax import lax
from jax.experimental import pallas as pl
from jax.experimental.pallas import tpu as pltpu
from jax.sharding import PartitionSpec as P

MESH = pl.DeviceIdType.MESH
F32 = jnp.float32
BF16 = jnp.bfloat16

HEAD_DIM = 64
WINDOW = 128
EPSILON = 1e-06
ROPE_BASE = 10000.0
MASK_VALUE = -1e30
RIM = 16
LN_ROWS = 256
CORES = 2


def dot(a, b, dims=((1,), (0,))):
    return lax.dot_general(a, b, (dims, ((), ())), preferred_element_type=F32)


def kernel(
    dims,
    tokens,
    norm_gain,
    w_value,
    w_gate,
    w_query,
    w_key,
    w_val,
    conv_taps,
    conv_gain,
    sink,
    w_oc,
    w_oa,
    cos_ref,
    sin_ref,
    mixed,
    log_total,
    tbuf,
    gain_buf,
    normed,
    w_a,
    w_b,
    o_w,
    gain_all,
    taps_buf,
    gpad,
    qz,
    kpad,
    kvpad,
    bias,
    fsend,
    asend,
    cbm,
    bm,
    tok_sem,
    send_sem,
    recv_sem,
):
    SEQS, T, D, X, Z, Y, TP = dims
    NSP = X * Z
    per_seq = T // LN_ROWS
    n_blocks = SEQS * per_seq
    sp, tp = lax.axis_index("sp"), lax.axis_index("tp")
    z, x = sp // X, sp % X
    y, c = tp // CORES, tp % CORES
    half_y = Y // 2
    yh, yl = y // half_y, y % half_y
    slot = c * Y + y

    def at_x(d):
        return (z * X + (x + d) % X, tp)

    def at_z(d):
        return (((z + d) % Z) * X + x, tp)

    def at_y(d):
        return (sp, ((y + d) % Y) * CORES + c)

    def at_tp(d):
        return (sp, (tp + d) % TP)

    partner = (sp, y * CORES + (1 - c))
    right = ((sp + 1) % NSP, tp)
    left = ((sp + NSP - 1) % NSP, tp)

    counter = [0]

    def ids(n):
        first = counter[0]
        counter[0] += n
        return first

    def remote(src, dst, i, device):
        return pltpu.make_async_remote_copy(
            src_ref=src,
            dst_ref=dst,
            send_sem=send_sem.at[i],
            recv_sem=recv_sem.at[i],
            device_id=device,
            device_id_type=MESH,
        )

    def start(copies):
        for cp in copies:
            cp.start()

    def arrived(copies):
        for cp in copies:
            cp.wait_recv()

    def tok_copy(i):
        s, r = i // per_seq, (i % per_seq) * LN_ROWS
        return pltpu.make_async_copy(
            tokens.at[s, pl.ds(pl.multiple_of(r, LN_ROWS), LN_ROWS)], tbuf.at[i % 3], tok_sem.at[i % 3]
        )

    tok_copy(0).start()
    tok_copy(1).start()

    barrier = pltpu.get_barrier_semaphore()
    greeted = (
        [at_x(d) for d in range(1, X)]
        + [at_z(d) for d in range(1, Z)]
        + [left, right]
        + [at_tp(d) for d in range(1, TP)]
    )
    for device in greeted:
        pl.semaphore_signal(barrier, inc=1, device_id=device, device_id_type=MESH)

    w_a[z, x] = jnp.concatenate([w_value[...], w_gate[...]], axis=1)
    w_b[z, x] = jnp.concatenate([w_query[...], w_key[...], w_val[...]], axis=1)
    o_w[c, yh, z, x, pl.ds(pl.multiple_of(yl * 256, 256), 256)] = jnp.concatenate(
        [w_oc[...], w_oa[...]], axis=0
    )
    gain_all[slot] = jnp.broadcast_to(conv_gain[...].astype(F32), (8, 128))
    taps_buf[...] = conv_taps[...].astype(F32)
    gain_buf[...] = jnp.broadcast_to(norm_gain[...].astype(F32), (16, D))
    key_i = lax.broadcasted_iota(jnp.int32, (WINDOW, 256), 0)
    query_i = lax.broadcasted_iota(jnp.int32, (WINDOW, 256), 1) % WINDOW
    bias[0] = jnp.where(key_i >= query_i, 0.0, MASK_VALUE)
    bias[1] = jnp.where(key_i <= query_i, 0.0, MASK_VALUE)

    i = ids(X - 1)
    in_1 = [remote(w_a.at[z, x], w_a.at[z, x], i + d - 1, at_x(d)) for d in range(1, X)]
    i = ids(Z - 1)
    in_1 += [remote(w_b.at[z, x], w_b.at[z, x], i + d - 1, at_z(d)) for d in range(1, Z)]
    i = ids(Z - 1)
    in_2 = [remote(w_a.at[z], w_a.at[z], i + d - 1, at_z(d)) for d in range(1, Z)]
    i = ids(X - 1)
    in_2 += [remote(w_b.at[:, x], w_b.at[:, x], i + d - 1, at_x(d)) for d in range(1, X)]
    i = ids(Y - 1)
    tile = o_w.at[c, yh, z, x, pl.ds(pl.multiple_of(yl * 256, 256), 256)]
    out_0 = [remote(tile, tile, i + d - 1, at_y(d)) for d in range(1, Y)]
    i = ids(TP - 1)
    gains = [remote(gain_all.at[slot], gain_all.at[slot], i + d - 1, at_tp(d)) for d in range(1, TP)]
    i = ids(X - 1)
    out_1 = [remote(o_w.at[c, 0, z, x], o_w.at[c, 0, z, x], i + d - 1, at_x(d)) for d in range(1, X)]
    i = ids(Z - 1)
    out_1 += [remote(o_w.at[c, 1, z, x], o_w.at[c, 1, z, x], i + d - 1, at_z(d)) for d in range(1, Z)]
    i = ids(Z - 1)
    out_2 = [remote(o_w.at[c, 0, z], o_w.at[c, 0, z], i + d - 1, at_z(d)) for d in range(1, Z)]
    i = ids(X - 1)
    out_2 += [remote(o_w.at[c, 1, :, x], o_w.at[c, 1, :, x], i + d - 1, at_x(d)) for d in range(1, X)]
    i = ids(2)
    pair_1 = [
        remote(o_w.at[c, 0, z], o_w.at[c, 0, z], i, partner),
        remote(o_w.at[c, 1, :, x], o_w.at[c, 1, :, x], i + 1, partner),
    ]
    i = ids(Z - 1)
    pair_2 = []
    for d in range(1, Z):
        row = o_w.at[c, 0, (z + Z - d) % Z]
        pair_2.append(remote(row, row, i + d - 1, partner))
    i = ids(X - 1)
    for d in range(1, X):
        column = o_w.at[c, 1, :, (x + X - d) % X]
        pair_2.append(remote(column, column, i + d - 1, partner))

    halo_i = ids(4 * SEQS)

    def halos(s):
        i = halo_i + 4 * s
        return [
            remote(gpad.at[s, pl.ds(RIM, RIM)], gpad.at[s, pl.ds(RIM + T, RIM)], i, left),
            remote(gpad.at[s, pl.ds(T, RIM)], gpad.at[s, pl.ds(0, RIM)], i + 1, right),
            remote(kvpad.at[s, pl.ds(WINDOW, WINDOW)], kvpad.at[s, pl.ds(WINDOW + T, WINDOW)], i + 2, left),
            remote(kvpad.at[s, pl.ds(T, WINDOW)], kvpad.at[s, pl.ds(0, WINDOW)], i + 3, right),
        ]

    conv_i = ids((TP - 1) * SEQS)
    attn_i = ids((TP - 1) * SEQS)

    def rows_of(device_tp):
        return pl.ds(pl.multiple_of(device_tp * 128, 128), 128)

    conv_lanes = pl.ds(pl.multiple_of(slot * 128, 128), 128)
    attn_lanes = pl.ds(pl.multiple_of(slot * 256 + 128, 128), 128)

    def conv_out_copies(s):
        return [
            remote(
                fsend.at[s, rows_of((tp + d) % TP)],
                cbm.at[s, :, conv_lanes],
                conv_i + (TP - 1) * s + d - 1,
                at_tp(d),
            )
            for d in range(1, TP)
        ]

    def attn_out_copies(s):
        return [
            remote(
                asend.at[s, rows_of((tp + d) % TP)],
                bm.at[s, :, attn_lanes],
                attn_i + (TP - 1) * s + d - 1,
                at_tp(d),
            )
            for d in range(1, TP)
        ]

    pl.semaphore_wait(barrier, len(greeted))
    start(in_1)
    start(out_0)
    start(gains)

    def ln_block(i, carry):
        buf = i % 3
        tok_copy(i).wait()

        @pl.when(i + 2 < n_blocks)
        def _():
            tok_copy(i + 2).start()

        def group(g, carry):
            at = pl.multiple_of(g * 16, 16)
            v = tbuf[buf, pl.ds(at, 16), :].astype(F32)
            mean = jnp.sum(v, axis=-1, keepdims=True) * (1.0 / D)
            centred = v - mean
            var = jnp.sum(centred * centred, axis=-1, keepdims=True) * (1.0 / D)
            out = centred * lax.rsqrt(var + EPSILON) * gain_buf[...]
            normed[pl.ds(pl.multiple_of(i * LN_ROWS, LN_ROWS) + at, 16), :] = out.astype(BF16)
            return carry

        return lax.fori_loop(0, LN_ROWS // 16, group, carry, unroll=4)

    first_part = n_blocks // 4
    lax.fori_loop(0, first_part, ln_block, 0)
    arrived(in_1)
    start(in_2)
    lax.fori_loop(first_part, n_blocks, ln_block, 0)
    arrived(in_2)
    arrived(out_0)
    start(out_1)

    lane = lax.broadcasted_iota(jnp.int32, (1, 128), 1)
    low_half = (lane % HEAD_DIM) < HEAD_DIM // 2
    low_head = lane < HEAD_DIM

    def swapped(v):
        return jnp.where(low_half, pltpu.roll(v, 96, 1), pltpu.roll(v, 32, 1))

    proj_rows = 256

    def project(s):
        def step(k, carry):
            r = pl.multiple_of(k * proj_rows, proj_rows)
            rows = normed[pl.ds(pl.multiple_of(s * T, T) + r, proj_rows), :]
            a = dot(rows, w_a[...].reshape(D, 256))
            gated = a[:, :128] * jax.nn.sigmoid(a[:, 128:])
            gpad[s, pl.ds(RIM + r, proj_rows), :] = gated.astype(BF16).astype(F32)
            b = dot(rows, w_b[...].reshape(D, 256))
            cosine = cos_ref[pl.ds(r, proj_rows), :]
            sine = sin_ref[pl.ds(r, proj_rows), :]
            q, kv = b[:, :128], b[:, 128:]
            q = (q * cosine + swapped(q) * sine) * (HEAD_DIM**-0.5)
            zero = jnp.zeros_like(q)
            q_0 = jnp.where(low_head, q, zero).astype(BF16)
            q_1 = jnp.where(low_head, zero, q).astype(BF16)
            for n in range(proj_rows // 128):
                blk = k * (proj_rows // 128) + n
                qz[s, blk, 0] = q_0[n * 128 : (n + 1) * 128]
                qz[s, blk, 1] = q_1[n * 128 : (n + 1) * 128]
            turned = kv * cosine + swapped(kv) * sine
            kpad[s, pl.ds(WINDOW + r, proj_rows), :] = jnp.where(
                low_head, turned, pltpu.roll(turned, 64, 1)
            ).astype(BF16)
            kvpad[s, pl.ds(WINDOW + r, proj_rows), :] = jnp.where(low_head, turned, kv).astype(BF16)
            return carry

        lax.fori_loop(0, T // proj_rows, step, 0)

    def convolve(s):
        arriving = halos(s)
        arriving[0].wait_recv()
        arriving[1].wait_recv()

        @pl.when(sp == 0)
        def _():
            gpad[s, pl.ds(0, RIM), :] = jnp.zeros((RIM, 128), F32)

        @pl.when(sp == NSP - 1)
        def _():
            gpad[s, pl.ds(RIM + T, RIM), :] = jnp.zeros((RIM, 128), F32)

        def chunk(k, carry):
            r = pl.multiple_of(k * 128, 128)
            total = jnp.zeros((128, 128), F32)
            for j in range(31):
                total = total + gpad[s, pl.ds(r + (j + 1), 128), :] * taps_buf[pl.ds(j, 1), :]
            fsend[s, pl.ds(r, 128), :] = total.astype(BF16)
            return carry

        lax.fori_loop(0, T // 128, chunk, 0)
        start(conv_out_copies(s))
        cbm[s, :, conv_lanes] = fsend[s, rows_of(tp), :]

    project(0)
    start(halos(0))

    def project_and_convolve(s, carry):
        project(s)
        start(halos(s))
        convolve(s - 1)
        return carry

    lax.fori_loop(1, SEQS, project_and_convolve, 0)
    arrived(out_1)
    start(out_2)
    start(pair_1)
    convolve(SEQS - 1)

    head_lane = lax.broadcasted_iota(jnp.int32, (1, 256), 1)
    sink_row = jnp.where(head_lane < 128, sink[0], sink[1])

    def widen(s, first):
        kv = kvpad[s, pl.ds(first, WINDOW), :].astype(F32)
        kpad[s, pl.ds(first, WINDOW), :] = jnp.where(low_head, kv, pltpu.roll(kv, 64, 1)).astype(BF16)

    def attend(s, carry):
        arriving = halos(s)
        arriving[2].wait_recv()
        arriving[3].wait_recv()
        widen(s, 0)
        widen(s, WINDOW + T)

        def block(b, carry):
            r = pl.multiple_of(b * 128, 128)
            keys = kpad[s, pl.ds(r, 384), :]
            scores = dot(keys, qz[s, b].reshape(256, 128), ((1,), (1,)))
            off_left = jnp.where((sp == 0) & (b == 0), MASK_VALUE, 0.0)
            off_right = jnp.where((sp == NSP - 1) & (b == T // 128 - 1), MASK_VALUE, 0.0)
            s_0 = scores[:128] + (bias[0] + off_left)
            s_1 = scores[128:256]
            s_2 = scores[256:] + (bias[1] + off_right)
            top = jnp.max(jnp.maximum(jnp.maximum(s_0, s_1), s_2), axis=0, keepdims=True)
            top = jnp.maximum(top, sink_row)
            e_0, e_1, e_2 = jnp.exp(s_0 - top), jnp.exp(s_1 - top), jnp.exp(s_2 - top)
            total = jnp.sum(e_0 + e_1 + e_2, axis=0, keepdims=True) + jnp.exp(sink_row - top)
            logs = top + jnp.log(total)
            log_total[s, :, pl.ds(r, 128)] = jnp.concatenate([logs[:, :128], logs[:, 128:]], axis=0)
            weights = jnp.concatenate([e_0.astype(BF16), e_1.astype(BF16), e_2.astype(BF16)], axis=0)
            out = dot(kvpad[s, pl.ds(r, 384), :], weights, ((0,), (0,)))
            out = out[64:] * (1.0 / total)
            both = jnp.concatenate([out[:, :128], out[:, 128:]], axis=0)
            asend[s, pl.ds(r, 128), :] = both.T.astype(BF16)
            return carry

        lax.fori_loop(0, T // 128, block, 0)
        start(attn_out_copies(s))
        bm[s, :, attn_lanes] = asend[s, rows_of(tp), :]
        return carry

    lax.fori_loop(0, SEQS - 1, attend, 0)
    arrived(out_2)
    start(pair_2)
    attend(SEQS - 1, 0)

    arrived(gains)

    def finish(s, carry):
        for cp in conv_out_copies(s):
            cp.wait_recv()

        def group(g, carry):
            at = pl.ds(pl.multiple_of(g * 16, 16), 16)
            v = cbm[s, at, :].astype(F32)
            mean = jnp.sum(v, axis=-1, keepdims=True) * (1.0 / (TP * 128))
            centred = v - mean
            var = jnp.sum(centred * centred, axis=-1, keepdims=True) * (1.0 / (TP * 128))
            scale = lax.rsqrt(var + EPSILON)
            for n in range(TP):
                u = centred[:, n * 128 : (n + 1) * 128] * scale * gain_all[n, 0:1, :]
                bm[s, at, n * 256 : n * 256 + 128] = jax.nn.silu(u).astype(BF16)
            return carry

        return lax.fori_loop(0, 128 // 16, group, carry, unroll=2)

    lax.fori_loop(0, SEQS, finish, 0)
    for s in range(SEQS):
        for cp in attn_out_copies(s):
            cp.wait_recv()
    arrived(pair_1)
    arrived(pair_2)

    def out_project(p, carry):
        zz, xx = p // (X // 2), (p % (X // 2)) * 2
        pieces = [
            jnp.concatenate([o_w[cc, hh, zz, xx], o_w[cc, hh, zz, xx + 1]], axis=1)
            for cc in range(CORES)
            for hh in range(2)
        ]
        acc = dot(bm[...].reshape(SEQS * 128, TP * 256), jnp.concatenate(pieces, axis=0))
        columns = pl.ds(pl.multiple_of(p * 256, 256), 256)
        mixed[:, :, columns] = acc.astype(BF16).reshape(SEQS, 128, 256)
        return carry

    lax.fori_loop(0, NSP // 2, out_project, 0)

    for cp in in_1 + in_2 + out_0 + gains + out_1 + out_2 + pair_1 + pair_2:
        cp.wait_send()

    def drain(s, carry):
        for cp in halos(s) + conv_out_copies(s) + attn_out_copies(s):
            cp.wait_send()
        return carry

    lax.fori_loop(0, SEQS, drain, 0)


def on_device(
    grid_shape,
    tokens,
    norm_gain,
    conv_value_weight,
    conv_gate_weight,
    query_weight,
    key_weight,
    value_weight,
    conv_taps,
    conv_gain,
    sink_logit,
    out_conv_weight,
    out_attn_weight,
):
    seqs, toks, width = tokens.shape
    xs, zs, ys, tps = grid_shape
    offset = lax.axis_index("sp") * toks
    positions = (offset + jnp.arange(toks, dtype=jnp.int32)).astype(F32)
    lanes = jnp.arange(128)
    half = HEAD_DIM // 2
    inverse = ROPE_BASE ** (-(lanes % half).astype(F32) / half)
    angles = positions[:, None] * inverse[None, :]
    cosine = jnp.cos(angles)
    sine = jnp.sin(angles) * jnp.where(lanes % HEAD_DIM < half, -1.0, 1.0)[None, :]

    n_copies = 4 * (xs - 1) + 4 * (zs - 1) + (ys - 1) + (tps - 1) + 2
    n_copies += (xs - 1) + (zs - 1) + 4 * seqs + 2 * (tps - 1) * seqs
    vmem = pl.BlockSpec(memory_space=pltpu.VMEM)
    call = pl.pallas_call(
        functools.partial(kernel, (seqs, toks, width, xs, zs, ys, tps)),
        out_shape=(
            jax.ShapeDtypeStruct((seqs, toks // tps, width), BF16),
            jax.ShapeDtypeStruct((seqs, 2, toks), F32),
        ),
        in_specs=[pl.BlockSpec(memory_space=pl.ANY)]
        + [vmem] * 8
        + [pl.BlockSpec(memory_space=pltpu.SMEM)]
        + [vmem] * 4,
        out_specs=(vmem, vmem),
        scratch_shapes=[
            pltpu.VMEM((3, LN_ROWS, width), BF16),
            pltpu.VMEM((16, width), F32),
            pltpu.VMEM((seqs * toks, width), BF16),
            pltpu.VMEM((zs, xs, 128, 256), BF16),
            pltpu.VMEM((zs, xs, 128, 256), BF16),
            pltpu.VMEM((CORES, 2, zs, xs, ys // 2 * 256, 128), BF16),
            pltpu.VMEM((tps, 8, 128), F32),
            pltpu.VMEM((31, 128), F32),
            pltpu.VMEM((seqs, toks + 2 * RIM, 128), F32),
            pltpu.VMEM((seqs, toks // 128, 2, 128, 128), BF16),
            pltpu.VMEM((seqs, toks + 2 * WINDOW, 128), BF16),
            pltpu.VMEM((seqs, toks + 2 * WINDOW, 128), BF16),
            pltpu.VMEM((2, WINDOW, 256), F32),
            pltpu.VMEM((seqs, toks, 128), BF16),
            pltpu.VMEM((seqs, toks, 128), BF16),
            pltpu.VMEM((seqs, toks // tps, tps * 128), BF16),
            pltpu.VMEM((seqs, toks // tps, tps * 256), BF16),
            pltpu.SemaphoreType.DMA((3,)),
            pltpu.SemaphoreType.DMA((n_copies,)),
            pltpu.SemaphoreType.DMA((n_copies,)),
        ],
        compiler_params=pltpu.CompilerParams(
            collective_id=0, has_side_effects=True, vmem_limit_bytes=63 * 2**20
        ),
        name="layer",
    )
    return call(
        tokens,
        norm_gain.reshape(1, -1),
        conv_value_weight,
        conv_gate_weight,
        query_weight,
        key_weight,
        value_weight,
        conv_taps,
        conv_gain.reshape(1, -1),
        sink_logit,
        out_conv_weight,
        out_attn_weight,
        cosine,
        sine,
    )


def solution(mesh):
    placed = (
        P(None, "sp", None),
        P(),
        P("sp", "tp"),
        P("sp", "tp"),
        P("sp", "tp"),
        P("sp", "tp"),
        P("sp", "tp"),
        P(None, "tp"),
        P("tp"),
        P("tp"),
        P("tp", "sp"),
        P("tp", "sp"),
    )
    xs = int(round(mesh.shape["sp"] ** 0.5))
    shape = (xs, mesh.shape["sp"] // xs, mesh.shape["tp"] // CORES, mesh.shape["tp"])
    return jax.shard_map(
        functools.partial(on_device, shape),
        mesh=mesh,
        in_specs=placed,
        out_specs=(P(None, ("sp", "tp"), None), P(None, "tp", "sp")),
        check_vma=False,
    )
```

```python
import functools

import jax
import jax.numpy as jnp
import numpy as np
from jax import lax
from jax.experimental import pallas as pl
from jax.experimental.pallas import tpu as pltpu
from jax.sharding import PartitionSpec as P

MESH = pl.DeviceIdType.MESH
F32 = jnp.float32
BF16 = jnp.bfloat16

HEAD_DIM = 64
WINDOW = 128
EPSILON = 1e-06
ROPE_BASE = 10000.0
MASK_VALUE = -1e30
RIM = 16
LN_ROWS = 256
CORES = 2
SLOTS = 6


def dot(a, b, dims=((1,), (0,))):
    return lax.dot_general(a, b, (dims, ((), ())), preferred_element_type=F32)


def kernel(
    dims,
    tokens,
    norm_gain,
    w_value,
    w_gate,
    w_query,
    w_key,
    w_val,
    conv_taps,
    conv_gain,
    sink,
    w_oc,
    w_oa,
    turns,
    mixed,
    log_total,
    tbuf,
    gain_buf,
    normed,
    w_a,
    w_b,
    o_w,
    gain_all,
    taps_buf,
    key_buf,
    gain_rows,
    taps_rows,
    conv_gain_row,
    turn_buf,
    cos_ref,
    sin_ref,
    gpad,
    qz,
    kpad,
    val_t,
    edges,
    bias,
    fsend,
    asend,
    cbm,
    bm,
    tok_sem,
    load_sem,
    send_sem,
    recv_sem,
):
    SEQS, T, D, X, Z, Y, TP = dims
    NSP = X * Z
    per_seq = T // LN_ROWS
    n_blocks = SEQS * per_seq
    sp, tp = lax.axis_index("sp"), lax.axis_index("tp")
    z, x = sp // X, sp % X
    y, c = tp // CORES, tp % CORES
    half_y = Y // 2
    yh, yl = y // half_y, y % half_y
    slot = c * Y + y

    def at_x(d):
        return (z * X + (x + d) % X, tp)

    def at_z(d):
        return (((z + d) % Z) * X + x, tp)

    def at_y(d):
        return (sp, ((y + d) % Y) * CORES + c)

    def at_tp(d):
        return (sp, (tp + d) % TP)

    partner = (sp, y * CORES + (1 - c))
    right = ((sp + 1) % NSP, tp)
    left = ((sp + NSP - 1) % NSP, tp)

    counter = [0]

    def ids(n):
        first = counter[0]
        counter[0] += n
        return first

    def remote(src, dst, i, device):
        return pltpu.make_async_remote_copy(
            src_ref=src,
            dst_ref=dst,
            send_sem=send_sem.at[i],
            recv_sem=recv_sem.at[i],
            device_id=device,
            device_id_type=MESH,
        )

    def start(copies):
        for cp in copies:
            cp.start()

    def group_of(i, pairs, whole):
        copies = [remote(src, dst, i, device) for src, dst, device in pairs]
        return copies, remote(whole, whole, i, right)

    def arrived(group):
        group[1].wait_recv()

    def left_here(group):
        group[1].wait_send()

    class Ring:
        def __init__(self, part, me, size, at):
            i = ids(6)
            ahead, behind = at(1), at(size - 1)
            lo, hi = part(me, 0), part(me, 1)
            self.direct = [remote(lo, lo, i, ahead)]
            self.relayed, self.late = [], [remote(hi, hi, i + 1, ahead)]
            if size == 2:
                return
            self.direct.append(remote(hi, hi, i + 2, behind))
            self.late.append(remote(lo, lo, i + 3, behind))
            near, far = part((me + size - 1) % size, 0), part((me + 1) % size, 1)
            self.passed = [near, far]
            self.rest = [part((me + size - 1) % size, 1), part((me + 1) % size, 0)]
            self.relayed = [remote(near, near, i + 4, ahead), remote(far, far, i + 5, behind)]

        def begin(self):
            start(self.direct)
            start(self.late)

        def relay(self):
            for cp in self.direct:
                cp.wait_recv()
            start(self.relayed)

        def finish(self):
            for cp in self.late + self.relayed:
                cp.wait_recv()

        def drain(self):
            for cp in self.direct + self.late + self.relayed:
                cp.wait_send()

    def tok_copy(i):
        seq, r = i // per_seq, (i % per_seq) * LN_ROWS
        return pltpu.make_async_copy(
            tokens.at[seq, pl.ds(pl.multiple_of(r, LN_ROWS), LN_ROWS)],
            tbuf.at[i % SLOTS],
            tok_sem.at[i % SLOTS],
        )

    barrier = pltpu.get_barrier_semaphore()
    greeted = (
        [at_x(d) for d in range(1, X)]
        + [at_z(d) for d in range(1, Z)]
        + [left, right]
        + [at_tp(d) for d in range(1, TP)]
    )
    for device in greeted:
        pl.semaphore_signal(barrier, inc=1, device_id=device, device_id_type=MESH)

    tile_at = pl.multiple_of(yl * 256, 256)
    wanted = [
        (w_value, w_a.at[z, x, :, pl.ds(0, 128)]),
        (w_gate, w_a.at[z, x, :, pl.ds(128, 128)]),
        (w_query, w_b.at[z, x, :, pl.ds(0, 128)]),
        (w_oc, o_w.at[c, yh, z, x, pl.ds(tile_at, 128)]),
        (w_oa, o_w.at[c, yh, z, x, pl.ds(tile_at + 128, 128)]),
        (w_key, key_buf.at[pl.ds(0, 64)]),
        (w_val, key_buf.at[pl.ds(64, 64)]),
        (conv_taps, taps_rows),
        (turns.at[0], turn_buf.at[0]),
        (turns.at[1], turn_buf.at[1]),
        (norm_gain, gain_rows),
        (conv_gain, conv_gain_row),
    ]
    loads = [pltpu.make_async_copy(a, b, load_sem.at[n]) for n, (a, b) in enumerate(wanted)]
    for n in (5, 6, 8, 9, 0, 1, 2, 3, 4, 7, 10, 11):
        loads[n].start()

    for n in range(SLOTS - 1):
        tok_copy(n).start()
    for n in (8, 9, 10):
        loads[n].wait()
    run = turn_buf.shape[1] - NSP - 32
    cos_s, sin_s = turn_buf[0, pl.ds(run + 32 + sp, 1), :], turn_buf[1, pl.ds(run + 32 + sp, 1), :]
    cos_b, sin_b = turn_buf[0, run : run + 32, :], turn_buf[1, run : run + 32, :]
    cos_bs, sin_bs = cos_b * cos_s - sin_b * sin_s, sin_b * cos_s + cos_b * sin_s
    low_half = (lax.broadcasted_iota(jnp.int32, (1, 128), 1) % HEAD_DIM) < HEAD_DIM // 2
    sign = jnp.where(low_half, -1.0, 1.0)

    def turn(n, carry):
        cos_a, sin_a = turn_buf[0, pl.ds(n, 1), :], turn_buf[1, pl.ds(n, 1), :]
        at = pl.ds(pl.multiple_of(n * 32, 32), 32)
        cos_ref[at, :] = cos_bs * cos_a - sin_bs * sin_a
        sin_ref[at, :] = (sin_bs * cos_a + cos_bs * sin_a) * sign
        return carry

    lax.fori_loop(0, T // 32, turn, 0, unroll=2)

    for n in (5, 6, 7):
        loads[n].wait()
    w_b[z, x, :, 128:256] = key_buf[...].astype(F32).T.astype(BF16)
    taps_buf[...] = taps_rows[...].astype(F32)
    for n in range(D // 128):
        gain_buf[:, n * 128 : (n + 1) * 128] = jnp.broadcast_to(
            gain_rows[n : n + 1, :].astype(F32), (16, 128)
        )
    loads[11].wait()
    gain_all[slot] = jnp.broadcast_to(conv_gain_row[...].astype(F32), (8, 128))
    key_i = lax.broadcasted_iota(jnp.int32, (WINDOW, 256), 0)
    query_i = lax.broadcasted_iota(jnp.int32, (WINDOW, 256), 1) % WINDOW
    bias[0] = jnp.where(key_i >= query_i, 0.0, MASK_VALUE)
    bias[1] = jnp.where(key_i <= query_i, 0.0, MASK_VALUE)

    half_x, half_z = X // 2, Z // 2
    in_1 = [
        group_of(ids(1), [(w_a.at[z, x], w_a.at[z, x], at_x(d)) for d in range(1, X)], w_a.at[0, pl.ds(0, X - 1)]),
        group_of(ids(1), [(w_b.at[z, x], w_b.at[z, x], at_z(d)) for d in range(1, Z)], w_b.at[pl.ds(0, Z - 1), 0]),
    ]
    in_2 = [
        Ring(lambda k, h: w_a.at[k, pl.ds(h * half_x, half_x)], z, Z, at_z),
        Ring(lambda k, h: w_b.at[pl.ds(h * half_z, half_z), k], x, X, at_x),
    ]
    tile = o_w.at[c, yh, z, x, pl.ds(tile_at, 256)]
    out_0 = group_of(ids(1), [(tile, tile, at_y(d)) for d in range(1, Y)], fsend.at[0, pl.ds(0, (Y - 1) * 256)])
    own_gain = gain_all.at[slot]
    gains = group_of(ids(1), [(own_gain, own_gain, at_tp(d)) for d in range(1, TP)], gain_all.at[pl.ds(0, TP - 1)])
    out_1 = [
        group_of(
            ids(1),
            [(o_w.at[c, 0, z, x], o_w.at[c, 0, z, x], at_x(d)) for d in range(1, X)],
            o_w.at[0, 0, 0, pl.ds(0, X - 1)],
        ),
        group_of(
            ids(1),
            [(o_w.at[c, 1, z, x], o_w.at[c, 1, z, x], at_z(d)) for d in range(1, Z)],
            o_w.at[0, 0, pl.ds(0, Z - 1), 0],
        ),
    ]
    out_2 = [
        Ring(lambda k, h: o_w.at[c, 0, k, pl.ds(h * half_x, half_x)], z, Z, at_z),
        Ring(lambda k, h: o_w.at[c, 1, pl.ds(h * half_z, half_z), k], x, X, at_x),
    ]

    def to_partner(d):
        row, column = o_w.at[c, 0, (z + d) % Z], o_w.at[c, 1, :, (x + d) % X]
        return [(row, row, partner), (column, column, partner)]

    pair_1 = group_of(ids(1), to_partner(0), o_w.at[0, 0, pl.ds(0, 2)])
    if X == 2:
        early, late = [], to_partner(1)
        late_whole = o_w.at[0, 0, pl.ds(0, 2)]
    else:
        passed = [ref for ring in out_2 for ref in ring.passed]
        early = [(ref, ref, partner) for ref in passed]
        rest = [ref for ring in out_2 for ref in ring.rest]
        late = [(ref, ref, partner) for ref in rest] + to_partner(2)
        late_whole = o_w.at[0, 0]
    pair_2 = group_of(ids(1), early, o_w.at[0, 0, pl.ds(0, 2)])
    pair_3 = group_of(ids(1), late, late_whole)

    rim_i, keys_i = ids(SEQS), ids(SEQS)

    def rims(s):
        return group_of(
            rim_i + s,
            [
                (gpad.at[s, pl.ds(RIM, RIM)], gpad.at[s, pl.ds(RIM + T, RIM)], left),
                (gpad.at[s, pl.ds(T, RIM)], gpad.at[s, pl.ds(0, RIM)], right),
            ],
            gpad.at[0, pl.ds(0, 2 * RIM)],
        )

    def edge_keys(s):
        return group_of(
            keys_i + s,
            [(edges.at[s, 1], edges.at[s, 3], left), (edges.at[s, 2], edges.at[s, 0], right)],
            edges.at[0, pl.ds(0, 2)],
        )

    conv_i, attn_i = ids(SEQS), ids(SEQS)
    peers_rows = fsend.at[0, pl.ds(0, (TP - 1) * 128)]

    def rows_of(device_tp):
        return pl.ds(pl.multiple_of(device_tp * 128, 128), 128)

    conv_lanes = pl.ds(pl.multiple_of(slot * 128, 128), 128)
    attn_lanes = pl.ds(pl.multiple_of(slot * 256 + 128, 128), 128)

    def conv_out_copies(s):
        return group_of(
            conv_i + s,
            [
                (fsend.at[s, rows_of((tp + d) % TP)], cbm.at[s, :, conv_lanes], at_tp(d))
                for d in range(1, TP)
            ],
            peers_rows,
        )

    def attn_out_copies(s):
        return group_of(
            attn_i + s,
            [
                (asend.at[s, rows_of((tp + d) % TP)], bm.at[s, :, attn_lanes], at_tp(d))
                for d in range(1, TP)
            ],
            peers_rows,
        )

    for n in range(5):
        loads[n].wait()
    with jax.named_scope("greet"):
        pl.semaphore_wait(barrier, len(greeted))
    for group in in_1:
        start(group[0])
    start(out_0[0])
    start(gains[0])

    def ln_block(i, carry):
        tok_copy(i).wait()

        @pl.when(i + SLOTS - 1 < n_blocks)
        def _():
            tok_copy(i + SLOTS - 1).start()

        def group(g, carry):
            at = pl.ds(pl.multiple_of(i * LN_ROWS, LN_ROWS) + pl.multiple_of(g * 16, 16), 16)
            v = tbuf[i % SLOTS, pl.ds(pl.multiple_of(g * 16, 16), 16), :].astype(F32)
            mean = jnp.sum(v, axis=-1, keepdims=True) * (1.0 / D)
            centred = v - mean
            var = jnp.sum(centred * centred, axis=-1, keepdims=True) * (1.0 / D)
            out = centred * lax.rsqrt(var + EPSILON) * gain_buf[...]
            normed[at, :] = out.astype(BF16)
            return carry

        return lax.fori_loop(0, LN_ROWS // 16, group, carry, unroll=16)

    cuts = (0, n_blocks * 3 // 8, n_blocks * 7 // 8, n_blocks)
    with jax.named_scope("norm_a"):
        lax.fori_loop(cuts[0], cuts[1], ln_block, 0)
    with jax.named_scope("wait_in_1"):
        for group in in_1:
            arrived(group)
    for ring in in_2:
        ring.begin()
    with jax.named_scope("norm_b"):
        lax.fori_loop(cuts[1], cuts[2], ln_block, 0)
    with jax.named_scope("wait_relay"):
        for ring in in_2:
            ring.relay()
    with jax.named_scope("wait_out_0"):
        arrived(out_0)
    for group in out_1:
        start(group[0])
    with jax.named_scope("norm_c"):
        lax.fori_loop(cuts[2], cuts[3], ln_block, 0)
    with jax.named_scope("wait_in_2"):
        for ring in in_2:
            ring.finish()

    lane = lax.broadcasted_iota(jnp.int32, (1, 128), 1)
    low_head = lane < HEAD_DIM

    def swapped(v):
        return jnp.where(low_half, pltpu.roll(v, 96, 1), pltpu.roll(v, 32, 1))

    def project(s, starts):
        n = 256 // len(starts)
        at = [pl.ds(pl.multiple_of(s * T + r, 128), n) for r in starts]
        rows = jnp.concatenate([normed[rs, :] for rs in at], axis=0)
        a = dot(rows, w_a[...].reshape(D, 256))
        gated = a[:, :128] * jax.nn.sigmoid(a[:, 128:])
        gated = gated.astype(BF16).astype(F32)
        b = dot(rows, w_b[...].reshape(D, 256))
        at = [pl.ds(pl.multiple_of(r, 128), n) for r in starts]
        cosine = jnp.concatenate([cos_ref[rs, :] for rs in at], axis=0)
        sine = jnp.concatenate([sin_ref[rs, :] for rs in at], axis=0)
        q, kv = b[:, :128], b[:, 128:]
        q = (q * cosine + swapped(q) * sine) * (HEAD_DIM**-0.5)
        zero = jnp.zeros_like(q)
        q_0 = jnp.where(low_head, q, zero).astype(BF16)
        q_1 = jnp.where(low_head, zero, q).astype(BF16)
        turned = kv * cosine + swapped(kv) * sine
        twice = jnp.where(low_head, turned, pltpu.roll(turned, 64, 1)).astype(BF16)
        kv = jnp.where(low_head, turned, kv).astype(BF16)
        for k in range(2):
            r = pl.multiple_of(starts[k] if len(starts) == 2 else starts[0] + k * 128, 128)
            part = slice(k * 128, (k + 1) * 128)
            gpad[s, pl.ds(RIM + r, 128), :] = gated[part]
            qz[s, r // 128, 0] = q_0[part]
            qz[s, r // 128, 1] = q_1[part]
            kpad[s, pl.ds(WINDOW + r, 128), :] = twice[part]
            val_t[s, :, pl.ds(WINDOW + r, 128)] = kv[part].T[64:]
            if len(starts) == 2:
                edges[s, k + 1] = kv[part]

    def convolve(s):
        with jax.named_scope("wait_rim"):
            arrived(rims(s))

        @pl.when(sp == 0)
        def _():
            gpad[s, pl.ds(0, RIM), :] = jnp.zeros((RIM, 128), F32)

        @pl.when(sp == NSP - 1)
        def _():
            gpad[s, pl.ds(RIM + T, RIM), :] = jnp.zeros((RIM, 128), F32)

        def chunk(k, carry):
            r = pl.multiple_of(k * 128, 128)
            total = jnp.zeros((128, 128), F32)
            for j in range(31):
                total = total + gpad[s, pl.ds(r + (j + 1), 128), :] * taps_buf[pl.ds(j, 1), :]
            fsend[s, pl.ds(r, 128), :] = total.astype(BF16)
            return carry

        with jax.named_scope("conv"):
            lax.fori_loop(0, T // 128, chunk, 0)
        start(conv_out_copies(s)[0])
        cbm[s, :, conv_lanes] = fsend[s, rows_of(tp), :]

    def project_edges(s, carry):
        project(s, (0, T - 128))
        return carry

    def send_edges(s, carry):
        start(edge_keys(s)[0])
        start(rims(s)[0])
        return carry

    def project_inner(k, carry):
        inner = T // 256 - 1
        project(k // inner, (128 + (k % inner) * 256,))
        return carry

    n_inner = SEQS * (T // 256 - 1)
    inner_cut = n_inner // 2
    with jax.named_scope("project_edges"):
        lax.fori_loop(0, SEQS, project_edges, 0, unroll=2)
    lax.fori_loop(0, SEQS, send_edges, 0)
    with jax.named_scope("project_a"):
        lax.fori_loop(0, inner_cut, project_inner, 0, unroll=3)
    with jax.named_scope("wait_out_1"):
        for group in out_1:
            arrived(group)
    with jax.named_scope("wait_rims"):
        for ring in out_2:
            ring.begin()
    start(pair_1[0])
    with jax.named_scope("project_b"):
        lax.fori_loop(inner_cut, n_inner, project_inner, 0, unroll=3)

    def each_convolve(s, carry):
        convolve(s)
        return carry

    lax.fori_loop(0, SEQS, each_convolve, 0)
    with jax.named_scope("wait_out_relay"):
        for ring in out_2:
            ring.relay()
    start(pair_2[0])

    head_lane = lax.broadcasted_iota(jnp.int32, (1, 256), 1)
    sink_row = jnp.where(head_lane < 128, sink[0], sink[1])

    def widen(s, e, first):
        kv = edges[s, e].astype(F32)
        kpad[s, pl.ds(first, WINDOW), :] = jnp.where(low_head, kv, pltpu.roll(kv, 64, 1)).astype(BF16)
        val_t[s, :, pl.ds(first, WINDOW)] = edges[s, e].T[64:]

    def attend(s, carry):
        @pl.when(s == SEQS - 1)
        def _():
            with jax.named_scope("wait_out_2"):
                for ring in out_2:
                    ring.finish()
            start(pair_3[0])

        with jax.named_scope("wait_keys"):
            arrived(edge_keys(s))
        widen(s, 0, 0)
        widen(s, 3, WINDOW + T)

        def block(b, carry):
            r = pl.multiple_of(b * 128, 128)
            keys = kpad[s, pl.ds(r, 384), :]
            scores = dot(keys, qz[s, b].reshape(256, 128), ((1,), (1,)))
            off_left = jnp.where((sp == 0) & (b == 0), MASK_VALUE, 0.0)
            off_right = jnp.where((sp == NSP - 1) & (b == T // 128 - 1), MASK_VALUE, 0.0)
            s_0 = scores[:128] + (bias[0] + off_left)
            s_1 = scores[128:256]
            s_2 = scores[256:] + (bias[1] + off_right)
            top = jnp.max(jnp.maximum(jnp.maximum(s_0, s_1), s_2), axis=0, keepdims=True)
            top = jnp.maximum(top, sink_row)
            e_0, e_1, e_2 = jnp.exp(s_0 - top), jnp.exp(s_1 - top), jnp.exp(s_2 - top)
            total = jnp.sum(e_0 + e_1 + e_2, axis=0, keepdims=True) + jnp.exp(sink_row - top)
            logs = top + jnp.log(total)
            log_total[s, :, pl.ds(r, 128)] = jnp.concatenate([logs[:, :128], logs[:, 128:]], axis=0)
            weights = jnp.concatenate([e_0.astype(BF16), e_1.astype(BF16), e_2.astype(BF16)], axis=0)
            out = dot(val_t[s, :, pl.ds(r, 384)], weights) * (1.0 / total)
            both = jnp.concatenate([out[:, :128], out[:, 128:]], axis=0)
            asend[s, pl.ds(r, 128), :] = both.astype(BF16).T
            return carry

        with jax.named_scope("attend"):
            lax.fori_loop(0, T // 128, block, 0, unroll=min(8, T // 128))
        start(attn_out_copies(s)[0])
        bm[s, :, attn_lanes] = asend[s, rows_of(tp), :]
        return carry

    lax.fori_loop(0, SEQS, attend, 0)

    arrived(gains)

    def finish(s):
        with jax.named_scope("wait_conv"):
            arrived(conv_out_copies(s))

        def group(g, carry):
            at = pl.ds(pl.multiple_of(g * 16, 16), 16)
            v = cbm[s, at, :].astype(F32)
            mean = jnp.sum(v, axis=-1, keepdims=True) * (1.0 / (TP * 128))
            centred = v - mean
            var = jnp.sum(centred * centred, axis=-1, keepdims=True) * (1.0 / (TP * 128))
            scale = lax.rsqrt(var + EPSILON)
            for n in range(TP):
                u = centred[:, n * 128 : (n + 1) * 128] * scale * gain_all[n, 0:1, :]
                bm[s, at, n * 256 : n * 256 + 128] = jax.nn.silu(u).astype(BF16)
            return carry

        with jax.named_scope("channel_norm"):
            lax.fori_loop(0, 128 // 16, group, 0, unroll=8)

    def out_rows(s, carry):
        finish(2 * s)
        finish(2 * s + 1)
        with jax.named_scope("wait_attn"):
            arrived(attn_out_copies(2 * s))
            arrived(attn_out_copies(2 * s + 1))

        @pl.when(s == 0)
        def _():
            with jax.named_scope("wait_pair"):
                arrived(pair_1)
                if X > 2:
                    arrived(pair_2)
                arrived(pair_3)

        def out_project(p, carry):
            zz, xx = p // (X // 2), (p % (X // 2)) * 2
            pieces = [
                jnp.concatenate([o_w[cc, hh, zz, xx], o_w[cc, hh, zz, xx + 1]], axis=1)
                for cc in range(CORES)
                for hh in range(2)
            ]
            rows = bm[pl.ds(2 * s, 2)].reshape(256, TP * 256)
            acc = dot(rows, jnp.concatenate(pieces, axis=0))
            columns = pl.ds(pl.multiple_of(p * 256, 256), 256)
            mixed[pl.ds(2 * s, 2), :, columns] = acc.astype(BF16).reshape(2, 128, 256)
            return carry

        with jax.named_scope("out_project"):
            lax.fori_loop(0, NSP // 2, out_project, 0, unroll=2)
        return carry

    lax.fori_loop(0, SEQS // 2, out_rows, 0)

    for group in in_1 + [out_0, gains] + out_1 + [pair_1, pair_3] + ([pair_2] if X > 2 else []):
        left_here(group)
    for ring in in_2 + out_2:
        ring.drain()

    def drain(s, carry):
        for group in (rims(s), edge_keys(s), conv_out_copies(s), attn_out_copies(s)):
            left_here(group)
        return carry

    lax.fori_loop(0, SEQS, drain, 0)


def on_device(
    grid_shape,
    tokens,
    norm_gain,
    conv_value_weight,
    conv_gate_weight,
    query_weight,
    key_weight,
    value_weight,
    conv_taps,
    conv_gain,
    sink_logit,
    out_conv_weight,
    out_attn_weight,
):
    seqs, toks, width = tokens.shape
    xs, zs, ys, tps = grid_shape
    n_sp = xs * zs
    half = HEAD_DIM // 2
    inverse = (ROPE_BASE ** (-np.arange(half, dtype=np.float32) / half)).astype(np.float32)
    parts = [np.arange(toks // 32) * 32, np.arange(32), np.arange(n_sp) * toks]
    angles = np.concatenate(parts)[:, None] * np.tile(inverse.astype(np.float64), 4)[None, :]
    turns = np.stack([np.cos(angles), np.sin(angles)]).astype(np.float32)

    n_copies = 2 + 12 + 2 + 2 + 12 + 3 + 4 * seqs
    vmem = pl.BlockSpec(memory_space=pltpu.VMEM)
    far = pl.BlockSpec(memory_space=pl.ANY)
    call = pl.pallas_call(
        functools.partial(kernel, (seqs, toks, width, xs, zs, ys, tps)),
        out_shape=(
            pltpu.VMEM((seqs, toks // tps, width), BF16),
            pltpu.VMEM((seqs, 2, toks), F32),
        ),
        in_specs=[far] * 9 + [pl.BlockSpec(memory_space=pltpu.SMEM)] + [far] * 3,
        out_specs=(vmem, vmem),
        scratch_shapes=[
            pltpu.VMEM((SLOTS, LN_ROWS, width), BF16),
            pltpu.VMEM((16, width), F32),
            pltpu.VMEM((seqs * toks, width), BF16),
            pltpu.VMEM((zs, xs, 128, 256), BF16),
            pltpu.VMEM((zs, xs, 128, 256), BF16),
            pltpu.VMEM((CORES, 2, zs, xs, ys // 2 * 256, 128), BF16),
            pltpu.VMEM((tps, 8, 128), F32),
            pltpu.VMEM((31, 128), F32),
            pltpu.VMEM((128, 128), BF16),
            pltpu.VMEM((width // 128, 128), BF16),
            pltpu.VMEM((31, 128), BF16),
            pltpu.VMEM((1, 128), BF16),
            pltpu.VMEM(turns.shape, F32),
            pltpu.VMEM((toks, 128), F32),
            pltpu.VMEM((toks, 128), F32),
            pltpu.VMEM((seqs, toks + 2 * RIM, 128), F32),
            pltpu.VMEM((seqs, toks // 128, 2, 128, 128), BF16),
            pltpu.VMEM((seqs, toks + 2 * WINDOW, 128), BF16),
            pltpu.VMEM((seqs, HEAD_DIM, toks + 2 * WINDOW), BF16),
            pltpu.VMEM((seqs, 4, WINDOW, 128), BF16),
            pltpu.VMEM((2, WINDOW, 256), F32),
            pltpu.VMEM((seqs, toks, 128), BF16),
            pltpu.VMEM((seqs, toks, 128), BF16),
            pltpu.VMEM((seqs, toks // tps, tps * 128), BF16),
            pltpu.VMEM((seqs, toks // tps, tps * 256), BF16),
            pltpu.SemaphoreType.DMA((SLOTS,)),
            pltpu.SemaphoreType.DMA((12,)),
            pltpu.SemaphoreType.DMA((n_copies,)),
            pltpu.SemaphoreType.DMA((n_copies,)),
        ],
        compiler_params=pltpu.CompilerParams(
            collective_id=0, has_side_effects=True, vmem_limit_bytes=54 * 2**20
        ),
        name="layer",
    )
    return call(
        tokens,
        norm_gain.reshape(-1, 128),
        conv_value_weight,
        conv_gate_weight,
        query_weight,
        key_weight.T,
        value_weight.T,
        conv_taps,
        conv_gain.reshape(1, -1),
        sink_logit,
        out_conv_weight,
        out_attn_weight,
        jnp.asarray(turns),
    )


def solution(mesh):
    placed = (
        P(None, "sp", None),
        P(),
        P("sp", "tp"),
        P("sp", "tp"),
        P("sp", "tp"),
        P("sp", "tp"),
        P("sp", "tp"),
        P(None, "tp"),
        P("tp"),
        P("tp"),
        P("tp", "sp"),
        P("tp", "sp"),
    )
    xs = int(round(mesh.shape["sp"] ** 0.5))
    shape = (xs, mesh.shape["sp"] // xs, mesh.shape["tp"] // CORES, mesh.shape["tp"])
    return jax.shard_map(
        functools.partial(on_device, shape),
        mesh=mesh,
        in_specs=placed,
        out_specs=(P(None, ("sp", "tp"), None), P(None, "tp", "sp")),
        check_vma=False,
    )
```

```python
import functools

import jax
import jax.numpy as jnp
import numpy as np
from jax import lax
from jax.experimental import pallas as pl
from jax.experimental.pallas import tpu as pltpu
from jax.sharding import PartitionSpec as P

MESH = pl.DeviceIdType.MESH
F32 = jnp.float32
BF16 = jnp.bfloat16

HEAD_DIM = 64
WINDOW = 128
EPSILON = 1e-06
ROPE_BASE = 10000.0
MASK_VALUE = -1e30
RIM = 16
LN_ROWS = 256
CORES = 2
SLOTS = 6


def dot(a, b, dims=((1,), (0,))):
    return lax.dot_general(a, b, (dims, ((), ())), preferred_element_type=F32)


def kernel(
    dims,
    tokens,
    norm_gain,
    w_value,
    w_gate,
    w_query,
    w_key,
    w_val,
    conv_taps,
    conv_gain,
    sink,
    w_oc,
    w_oa,
    turns,
    mixed,
    log_total,
    tbuf,
    gain_buf,
    normed,
    w_a,
    w_b,
    o_w,
    gain_all,
    taps_buf,
    key_buf,
    gain_rows,
    taps_rows,
    conv_gain_row,
    turn_buf,
    cos_ref,
    sin_ref,
    gpad,
    qz,
    kpad,
    val_t,
    edges,
    bias,
    score_buf,
    weight_buf,
    partial_out,
    fsend,
    asend,
    cbm,
    bm,
    tok_sem,
    load_sem,
    send_sem,
    recv_sem,
):
    SEQS, T, D, X, Z, Y, TP = dims
    NSP = X * Z
    per_seq = T // LN_ROWS
    n_blocks = SEQS * per_seq
    sp, tp = lax.axis_index("sp"), lax.axis_index("tp")
    z, x = sp // X, sp % X
    y, c = tp // CORES, tp % CORES
    slot = c * Y + y
    own_rows = pl.ds(pl.multiple_of(y * 128, 128), 128)

    def at_x(d):
        return (z * X + (x + d) % X, tp)

    def at_z(d):
        return (((z + d) % Z) * X + x, tp)

    def at_y(d):
        return (sp, ((y + d) % Y) * CORES + c)

    def at_tp(d):
        return (sp, (tp + d) % TP)

    partner = (sp, y * CORES + (1 - c))
    right = ((sp + 1) % NSP, tp)
    left = ((sp + NSP - 1) % NSP, tp)

    counter = [0]

    def ids(n):
        first = counter[0]
        counter[0] += n
        return first

    def remote(src, dst, i, device):
        return pltpu.make_async_remote_copy(
            src_ref=src,
            dst_ref=dst,
            send_sem=send_sem.at[i],
            recv_sem=recv_sem.at[i],
            device_id=device,
            device_id_type=MESH,
        )

    def start(copies):
        for cp in copies:
            cp.start()

    def group_of(i, pairs, whole):
        copies = [remote(src, dst, i, device) for src, dst, device in pairs]
        return copies, remote(whole, whole, i, right)

    def arrived(group):
        group[1].wait_recv()

    def left_here(group):
        group[1].wait_send()

    class Ring:
        def __init__(self, part, whole, me, size, at):
            i = ids(6)
            before, after = (me + size - 1) % size, (me + 1) % size

            def half(n, k, h, d):
                return group_of(i + n, [(ref, ref, at(d)) for ref in part(k, h)], whole)

            self.direct = [half(0, me, 0, 1)]
            self.relayed, self.late = [], [half(1, me, 1, 1)]
            self.passed, self.rest = [], []
            if size == 2:
                return
            self.direct.append(half(2, me, 1, size - 1))
            self.late.append(half(3, me, 0, size - 1))
            self.relayed = [half(4, before, 0, 1), half(5, after, 1, size - 1)]
            self.passed = part(before, 0) + part(after, 1)
            self.rest = part(before, 1) + part(after, 0)

        def begin(self):
            for group in self.direct + self.late:
                start(group[0])

        def relay(self):
            for group in self.direct:
                arrived(group)
            for group in self.relayed:
                start(group[0])

        def near(self):
            for group in self.late:
                arrived(group)

        def finish(self):
            for group in self.relayed:
                arrived(group)

        def drain(self):
            for group in self.direct + self.late + self.relayed:
                left_here(group)

    def tok_copy(i):
        seq, r = i // per_seq, (i % per_seq) * LN_ROWS
        return pltpu.make_async_copy(
            tokens.at[seq, pl.ds(pl.multiple_of(r, LN_ROWS), LN_ROWS)],
            tbuf.at[i % SLOTS],
            tok_sem.at[i % SLOTS],
        )

    barrier = pltpu.get_barrier_semaphore()
    greeted = (
        [at_x(d) for d in range(1, X)]
        + [at_z(d) for d in range(1, Z)]
        + [left, right]
        + [at_tp(d) for d in range(1, TP)]
    )
    for device in greeted:
        pl.semaphore_signal(barrier, inc=1, device_id=device, device_id_type=MESH)

    wanted = [
        (w_value, w_a.at[z, x, :, pl.ds(0, 128)]),
        (w_gate, w_a.at[z, x, :, pl.ds(128, 128)]),
        (w_query, w_b.at[z, x, :, pl.ds(0, 128)]),
        (w_oc, o_w.at[c, 0, z, x, own_rows]),
        (w_oa, o_w.at[c, 1, z, x, own_rows]),
        (w_key, key_buf.at[pl.ds(0, 64)]),
        (w_val, key_buf.at[pl.ds(64, 64)]),
        (conv_taps, taps_rows),
        (turns.at[0], turn_buf.at[0]),
        (turns.at[1], turn_buf.at[1]),
        (norm_gain, gain_rows),
        (conv_gain, conv_gain_row),
    ]
    loads = [pltpu.make_async_copy(a, b, load_sem.at[n]) for n, (a, b) in enumerate(wanted)]
    for n in (5, 6, 8, 9, 0, 1, 2, 3, 4, 7, 10, 11):
        loads[n].start()

    for n in range(SLOTS - 1):
        tok_copy(n).start()
    for n in (8, 9, 10):
        loads[n].wait()
    run = turn_buf.shape[1] - NSP - 32
    cos_s, sin_s = turn_buf[0, pl.ds(run + 32 + sp, 1), :], turn_buf[1, pl.ds(run + 32 + sp, 1), :]
    cos_b, sin_b = turn_buf[0, run : run + 32, :], turn_buf[1, run : run + 32, :]
    cos_bs, sin_bs = cos_b * cos_s - sin_b * sin_s, sin_b * cos_s + cos_b * sin_s
    low_half = (lax.broadcasted_iota(jnp.int32, (1, 128), 1) % HEAD_DIM) < HEAD_DIM // 2
    sign = jnp.where(low_half, -1.0, 1.0)

    def turn(n, carry):
        cos_a, sin_a = turn_buf[0, pl.ds(n, 1), :], turn_buf[1, pl.ds(n, 1), :]
        at = pl.ds(pl.multiple_of(n * 32, 32), 32)
        cos_ref[at, :] = cos_bs * cos_a - sin_bs * sin_a
        sin_ref[at, :] = (sin_bs * cos_a + cos_bs * sin_a) * sign
        return carry

    lax.fori_loop(0, T // 32, turn, 0, unroll=2)

    for n in (5, 6, 7):
        loads[n].wait()
    w_b[z, x, :, 128:256] = key_buf[...].astype(F32).T.astype(BF16)
    taps_buf[...] = taps_rows[...].astype(F32)
    for n in range(D // 128):
        gain_buf[:, n * 128 : (n + 1) * 128] = jnp.broadcast_to(
            gain_rows[n : n + 1, :].astype(F32), (16, 128)
        )
    loads[11].wait()
    gain_all[slot] = jnp.broadcast_to(conv_gain_row[...].astype(F32), (8, 128))
    key_i = lax.broadcasted_iota(jnp.int32, (WINDOW, 256), 0)
    query_i = lax.broadcasted_iota(jnp.int32, (WINDOW, 256), 1) % WINDOW
    bias[0] = jnp.where(key_i >= query_i, 0.0, MASK_VALUE)
    bias[1] = jnp.where(key_i <= query_i, 0.0, MASK_VALUE)

    half_x, half_z = X // 2, Z // 2
    in_1 = [
        group_of(ids(1), [(w_a.at[z, x], w_a.at[z, x], at_x(d)) for d in range(1, X)], w_a.at[0, pl.ds(0, X - 1)]),
        group_of(ids(1), [(w_b.at[z, x], w_b.at[z, x], at_z(d)) for d in range(1, Z)], w_b.at[pl.ds(0, Z - 1), 0]),
    ]
    rows_half = 128 // 2

    def others(block, me, size, h):
        if size == 2:
            return [block(1 - me).at[pl.ds(h * rows_half, rows_half)]]
        opposite = block((me + 2) % size).at[pl.ds(h * rows_half, rows_half)]
        return [block((me + 1 + 2 * h) % size), opposite]

    half_rows = w_a.at[0, 0, pl.ds(0, rows_half)]
    most_rows = w_a.at[0, pl.ds(0, X - 1), pl.ds(0, rows_half)]
    in_own = [
        Ring(lambda k, h: [w_a.at[k, x, pl.ds(h * rows_half, rows_half)]], half_rows, z, Z, at_z),
        Ring(lambda k, h: [w_b.at[z, k, pl.ds(h * rows_half, rows_half)]], half_rows, x, X, at_x),
    ]
    in_2 = [
        Ring(lambda k, h: others(lambda n: w_a.at[k, n], x, X, h), most_rows, z, Z, at_z),
        Ring(lambda k, h: others(lambda n: w_b.at[n, k], z, Z, h), most_rows, x, X, at_x),
    ]
    own_gain = gain_all.at[slot]
    gains = group_of(ids(1), [(own_gain, own_gain, at_tp(d)) for d in range(1, TP)], gain_all.at[pl.ds(0, TP - 1)])
    tile_0, tile_1 = o_w.at[c, 0, z, x, own_rows], o_w.at[c, 1, z, x, own_rows]
    out_0 = [
        group_of(ids(1), [(tile_0, tile_0, at_x(d)) for d in range(1, X)], fsend.at[0, pl.ds(0, (X - 1) * 128)]),
        group_of(ids(1), [(tile_1, tile_1, at_z(d)) for d in range(1, Z)], fsend.at[0, pl.ds(0, (Z - 1) * 128)]),
    ]
    row_0, column_1 = o_w.at[c, 0, z, :, own_rows], o_w.at[c, 1, :, x, own_rows]
    out_1 = [
        group_of(ids(1), [(row_0, row_0, at_y(d)) for d in range(1, Y)], o_w.at[0, 0, 0, :, pl.ds(0, (Y - 1) * 128)]),
        group_of(
            ids(1), [(column_1, column_1, at_y(d)) for d in range(1, Y)], o_w.at[0, 0, :, 0, pl.ds(0, (Y - 1) * 128)]
        ),
    ]
    out_2 = [
        Ring(lambda k, h: [o_w.at[c, 0, k, pl.ds(h * half_x, half_x)]], o_w.at[0, 0, 0, pl.ds(0, half_x)], z, Z, at_z),
        Ring(lambda k, h: [o_w.at[c, 1, pl.ds(h * half_z, half_z), k]], o_w.at[0, 0, 0, pl.ds(0, half_x)], x, X, at_x),
    ]

    def to_partner(d):
        row, column = o_w.at[c, 0, (z + d) % Z], o_w.at[c, 1, :, (x + d) % X]
        return [(row, row, partner), (column, column, partner)]

    pair_1 = group_of(ids(1), to_partner(0), o_w.at[0, 0, pl.ds(0, 2)])
    pairs = [pair_1]
    if X == 2:
        pair_4 = group_of(ids(1), to_partner(1), o_w.at[0, 0, pl.ds(0, 2)])
        pairs += [pair_4]
    else:
        passed = [(ref, ref, partner) for ring in out_2 for ref in ring.passed]
        rest = [(ref, ref, partner) for ring in out_2 for ref in ring.rest]
        pair_2 = group_of(ids(1), passed, o_w.at[0, 0, pl.ds(0, 2)])
        pair_3 = group_of(ids(1), rest, o_w.at[0, 0, pl.ds(0, 2)])
        pair_4 = group_of(ids(1), to_partner(2), o_w.at[0, 0, pl.ds(0, 2)])
        pairs += [pair_2, pair_3, pair_4]

    rim_i, keys_i = ids(SEQS), ids(SEQS)

    def rims(s):
        return group_of(
            rim_i + s,
            [
                (gpad.at[s, pl.ds(RIM, RIM)], gpad.at[s, pl.ds(RIM + T, RIM)], left),
                (gpad.at[s, pl.ds(T, RIM)], gpad.at[s, pl.ds(0, RIM)], right),
            ],
            gpad.at[0, pl.ds(0, 2 * RIM)],
        )

    def edge_keys(s):
        return group_of(
            keys_i + s,
            [(edges.at[s, 1], edges.at[s, 3], left), (edges.at[s, 2], edges.at[s, 0], right)],
            edges.at[0, pl.ds(0, 2)],
        )

    conv_i, attn_i = ids(SEQS), ids(SEQS)
    peers_rows = fsend.at[0, pl.ds(0, (TP - 1) * 128)]

    def rows_of(device_tp):
        return pl.ds(pl.multiple_of(device_tp * 128, 128), 128)

    conv_lanes = pl.ds(pl.multiple_of(slot * 128, 128), 128)
    attn_lanes = pl.ds(pl.multiple_of(c * (Y * 256) + (Y + y) * 128, 128), 128)

    def conv_out_copies(s):
        return group_of(
            conv_i + s,
            [
                (fsend.at[s, rows_of((tp + d) % TP)], cbm.at[s, :, conv_lanes], at_tp(d))
                for d in range(1, TP)
            ],
            peers_rows,
        )

    def attn_out_copies(s):
        return group_of(
            attn_i + s,
            [
                (asend.at[s, rows_of((tp + d) % TP)], bm.at[s, :, attn_lanes], at_tp(d))
                for d in range(1, TP)
            ],
            peers_rows,
        )

    for n in range(5):
        loads[n].wait()
    with jax.named_scope("greet"):
        pl.semaphore_wait(barrier, len(greeted))
    for group in in_1:
        start(group[0])
    for ring in in_own:
        ring.begin()

    def ln_block(i, carry):
        tok_copy(i).wait()

        @pl.when(i + SLOTS - 1 < n_blocks)
        def _():
            tok_copy(i + SLOTS - 1).start()

        def group(g, carry):
            at = pl.ds(pl.multiple_of(i * LN_ROWS, LN_ROWS) + pl.multiple_of(g * 16, 16), 16)
            v = tbuf[i % SLOTS, pl.ds(pl.multiple_of(g * 16, 16), 16), :].astype(F32)
            mean = jnp.sum(v, axis=-1, keepdims=True) * (1.0 / D)
            centred = v - mean
            var = jnp.sum(centred * centred, axis=-1, keepdims=True) * (1.0 / D)
            out = centred * lax.rsqrt(var + EPSILON) * gain_buf[...]
            normed[at, :] = out.astype(BF16)
            return carry

        return lax.fori_loop(0, LN_ROWS // 16, group, carry, unroll=16)

    def norm_blocks(first, last):
        with jax.named_scope("norm"):
            lax.fori_loop(n_blocks * first // 16, n_blocks * last // 16, ln_block, 0)

    norm_blocks(0, 2)
    for group in out_0:
        start(group[0])
    start(gains[0])
    norm_blocks(2, 6)
    with jax.named_scope("wait_in_1"):
        for group in in_1:
            arrived(group)
    for ring in in_2:
        ring.begin()
    with jax.named_scope("wait_own"):
        for ring in in_own:
            ring.relay()
    norm_blocks(6, 9)
    with jax.named_scope("wait_out_0"):
        for group in out_0:
            arrived(group)
    for group in out_1:
        start(group[0])
    norm_blocks(9, 13)
    with jax.named_scope("wait_relay"):
        for ring in in_2:
            ring.relay()
    norm_blocks(13, 16)
    with jax.named_scope("wait_in_2"):
        for ring in in_own + in_2:
            ring.near()
            ring.finish()

    lane = lax.broadcasted_iota(jnp.int32, (1, 128), 1)
    low_head = lane < HEAD_DIM

    def swapped(v):
        return jnp.where(low_half, pltpu.roll(v, 96, 1), pltpu.roll(v, 32, 1))

    def project(s, starts):
        n = 256 // len(starts)
        at = [pl.ds(pl.multiple_of(s * T + r, 128), n) for r in starts]
        rows = jnp.concatenate([normed[rs, :] for rs in at], axis=0)
        a = dot(rows, w_a[...].reshape(D, 256))
        gated = a[:, :128] * jax.nn.sigmoid(a[:, 128:])
        gated = gated.astype(BF16).astype(F32)
        b = dot(rows, w_b[...].reshape(D, 256))
        at = [pl.ds(pl.multiple_of(r, 128), n) for r in starts]
        cosine = jnp.concatenate([cos_ref[rs, :] for rs in at], axis=0)
        sine = jnp.concatenate([sin_ref[rs, :] for rs in at], axis=0)
        q, kv = b[:, :128], b[:, 128:]
        q = (q * cosine + swapped(q) * sine) * (HEAD_DIM**-0.5)
        zero = jnp.zeros_like(q)
        q_0 = jnp.where(low_head, q, zero).astype(BF16)
        q_1 = jnp.where(low_head, zero, q).astype(BF16)
        turned = kv * cosine + swapped(kv) * sine
        twice = jnp.where(low_head, turned, pltpu.roll(turned, 64, 1)).astype(BF16)
        kv = jnp.where(low_head, turned, kv).astype(BF16)
        for k in range(2):
            r = pl.multiple_of(starts[k] if len(starts) == 2 else starts[0] + k * 128, 128)
            part = slice(k * 128, (k + 1) * 128)
            gpad[s, pl.ds(RIM + r, 128), :] = gated[part]
            qz[s, r // 128, 0] = q_0[part]
            qz[s, r // 128, 1] = q_1[part]
            kpad[s, pl.ds(WINDOW + r, 128), :] = twice[part]
            val_t[s, :, pl.ds(WINDOW + r, 128)] = kv[part].T[64:]
            if len(starts) == 2:
                edges[s, k + 1] = kv[part]

    def convolve(s):
        with jax.named_scope("wait_rim"):
            arrived(rims(s))

        @pl.when(sp == 0)
        def _():
            gpad[s, pl.ds(0, RIM), :] = jnp.zeros((RIM, 128), F32)

        @pl.when(sp == NSP - 1)
        def _():
            gpad[s, pl.ds(RIM + T, RIM), :] = jnp.zeros((RIM, 128), F32)

        def chunk(k, carry):
            r = pl.multiple_of(k * 128, 128)
            total = jnp.zeros((128, 128), F32)
            for j in range(31):
                total = total + gpad[s, pl.ds(r + (j + 1), 128), :] * taps_buf[pl.ds(j, 1), :]
            fsend[s, pl.ds(r, 128), :] = total.astype(BF16)
            return carry

        with jax.named_scope("conv"):
            lax.fori_loop(0, T // 128, chunk, 0)
        start(conv_out_copies(s)[0])
        cbm[s, :, conv_lanes] = fsend[s, rows_of(tp), :]

    def project_edges(k, carry):
        for s in (2 * k, 2 * k + 1):
            project(s, (0, T - 128))
        for s in (2 * k, 2 * k + 1):
            start(rims(s)[0])
        for s in (2 * k, 2 * k + 1):
            start(edge_keys(s)[0])
        return carry

    inner = T // 256 - 1

    with jax.named_scope("project_edges"):
        lax.fori_loop(0, SEQS // 2, project_edges, 0)
    with jax.named_scope("wait_out_1"):
        for group in out_1:
            arrived(group)
    for ring in out_2:
        ring.begin()
    start(pair_1[0])

    def project_inner(s):
        def step(k, carry):
            project(s, (128 + k * 256,))
            return carry

        with jax.named_scope("project"):
            lax.fori_loop(0, inner, step, 0, unroll=inner)

    head_lane = lax.broadcasted_iota(jnp.int32, (1, 256), 1)
    sink_row = jnp.where(head_lane < 128, sink[0], sink[1])

    def widen(s, e, first):
        kv = edges[s, e].astype(F32)
        kpad[s, pl.ds(first, WINDOW), :] = jnp.where(low_head, kv, pltpu.roll(kv, 64, 1)).astype(BF16)
        val_t[s, :, pl.ds(first, WINDOW)] = edges[s, e].T[64:]

    blocks = T // 128

    def attend(s):
        with jax.named_scope("wait_keys"):
            arrived(edge_keys(s))
        widen(s, 0, 0)
        widen(s, 3, WINDOW + T)

        tops, totals = {}, {}

        def score(b):
            keys = kpad[s, pl.ds(b * 128, 384), :]
            scores = dot(keys, qz[s, b].reshape(256, 128), ((1,), (1,)))
            low, high = bias[0], bias[1]
            if b == 0:
                low = low + jnp.where(sp == 0, MASK_VALUE, 0.0)
            if b == blocks - 1:
                high = high + jnp.where(sp == NSP - 1, MASK_VALUE, 0.0)
            s_0, s_1, s_2 = scores[:128] + low, scores[128:256], scores[256:] + high
            top = jnp.max(jnp.maximum(jnp.maximum(s_0, s_1), s_2), axis=0, keepdims=True)
            tops[b] = jnp.maximum(top, sink_row)
            for n, part in enumerate((s_0, s_1, s_2)):
                score_buf[b % 2, n] = part

        def weigh(b):
            top = tops[b]
            e_0, e_1, e_2 = (jnp.exp(score_buf[b % 2, n] - top) for n in range(3))
            total = jnp.sum(e_0 + e_1 + e_2, axis=0, keepdims=True) + jnp.exp(sink_row - top)
            totals[b] = total
            logs = top + jnp.log(total)
            log_total[s, :, pl.ds(b * 128, 128)] = jnp.concatenate([logs[:, :128], logs[:, 128:]], axis=0)
            for n, part in enumerate((e_0, e_1, e_2)):
                weight_buf[b % 2, n] = part.astype(BF16)

        def collect(b):
            weights = weight_buf[b % 2].reshape(384, 256)
            out = dot(val_t[s, :, pl.ds(b * 128, 384)], weights) * (1.0 / totals[b])
            both = jnp.concatenate([out[:, :128], out[:, 128:]], axis=0)
            asend[s, pl.ds(b * 128, 128), :] = both.astype(BF16).T

        with jax.named_scope("attend"):
            for b in range(blocks + 2):
                if b < blocks:
                    score(b)
                if 0 <= b - 1 < blocks:
                    weigh(b - 1)
                if b >= 2:
                    collect(b - 2)
        start(attn_out_copies(s)[0])
        bm[s, :, attn_lanes] = asend[s, rows_of(tp), :]

    def sequence(s, carry):
        project_inner(s)

        @pl.when(s == SEQS - 1)
        def _():
            with jax.named_scope("wait_out_2"):
                for ring in out_2:
                    ring.finish()
            start(pair_4[0])

        convolve(s)

        @pl.when(s == min(1, SEQS - 1))
        def _():
            with jax.named_scope("wait_out_relay"):
                for ring in out_2:
                    ring.relay()
            if X > 2:
                start(pair_2[0])

        @pl.when(s == min(2, SEQS - 1))
        def _():
            with jax.named_scope("wait_out_near"):
                for ring in out_2:
                    ring.near()
            if X > 2:
                start(pair_3[0])

        attend(s)
        return carry

    lax.fori_loop(0, SEQS, sequence, 0)
    arrived(gains)

    def finish(s):
        with jax.named_scope("wait_conv"):
            arrived(conv_out_copies(s))

        def group(g, carry):
            at = pl.ds(pl.multiple_of(g * 16, 16), 16)
            v = cbm[s, at, :].astype(F32)
            mean = jnp.sum(v, axis=-1, keepdims=True) * (1.0 / (TP * 128))
            centred = v - mean
            var = jnp.sum(centred * centred, axis=-1, keepdims=True) * (1.0 / (TP * 128))
            scale = lax.rsqrt(var + EPSILON)
            for n in range(TP):
                u = centred[:, n * 128 : (n + 1) * 128] * scale * gain_all[n, 0:1, :]
                first = n // Y * (Y * 256) + n % Y * 128
                bm[s, at, first : first + 128] = jax.nn.silu(u).astype(BF16)
            return carry

        with jax.named_scope("channel_norm"):
            lax.fori_loop(0, 128 // 16, group, 0, unroll=8)

    def out_columns(p, h):
        zz, xx = p // (X // 2), (p % (X // 2)) * 2
        pieces = [
            jnp.concatenate([o_w[cc, hh, zz, xx], o_w[cc, hh, zz, xx + 1]], axis=1)
            for cc in range(CORES)
            for hh in h
        ]
        return jnp.concatenate(pieces, axis=0)

    columns_of = lambda p: pl.ds(pl.multiple_of(p * 256, 256), 256)
    first_rows = SEQS // 2

    for s in range(SEQS):
        finish(s)
        if s == first_rows - 1:
            with jax.named_scope("wait_pair"):
                for group in pairs:
                    arrived(group)
            with jax.named_scope("wait_attn"):
                for n in range(first_rows):
                    arrived(attn_out_copies(n))

            def out_whole(p, carry):
                rows = bm[:first_rows].reshape(first_rows * 128, TP * 256)
                acc = dot(rows, out_columns(p, (0, 1)))
                mixed[:first_rows, :, columns_of(p)] = acc.astype(BF16).reshape(first_rows, 128, 256)
                return carry

            with jax.named_scope("out_whole"):
                lax.fori_loop(0, NSP // 2, out_whole, 0, unroll=2)

    n_late = SEQS - first_rows
    branch = Y * 128

    def late_rows(h):
        first = [(2 * cc + h) * branch for cc in range(CORES)]
        lanes = [bm[first_rows:, :, k : k + branch].reshape(n_late * 128, branch) for k in first]
        return jnp.concatenate(lanes, axis=1)

    def out_conv(p, carry):
        partial_out[p] = dot(late_rows(0), out_columns(p, (0,)))
        return carry

    with jax.named_scope("out_conv"):
        lax.fori_loop(0, NSP // 2, out_conv, 0, unroll=2)
    with jax.named_scope("wait_attn"):
        for n in range(first_rows, SEQS):
            arrived(attn_out_copies(n))

    def out_attn(p, carry):
        acc = partial_out[p] + dot(late_rows(1), out_columns(p, (1,)))
        mixed[first_rows:, :, columns_of(p)] = acc.astype(BF16).reshape(n_late, 128, 256)
        return carry

    with jax.named_scope("out_attn"):
        lax.fori_loop(0, NSP // 2, out_attn, 0, unroll=2)

    for group in in_1 + [gains] + out_0 + out_1 + pairs:
        left_here(group)
    for ring in in_own + in_2 + out_2:
        ring.drain()

    def drain(s, carry):
        for group in (rims(s), edge_keys(s), conv_out_copies(s), attn_out_copies(s)):
            left_here(group)
        return carry

    lax.fori_loop(0, SEQS, drain, 0)


def on_device(
    grid_shape,
    tokens,
    norm_gain,
    conv_value_weight,
    conv_gate_weight,
    query_weight,
    key_weight,
    value_weight,
    conv_taps,
    conv_gain,
    sink_logit,
    out_conv_weight,
    out_attn_weight,
):
    seqs, toks, width = tokens.shape
    xs, zs, ys, tps = grid_shape
    n_sp = xs * zs
    half = HEAD_DIM // 2
    inverse = (ROPE_BASE ** (-np.arange(half, dtype=np.float32) / half)).astype(np.float32)
    parts = [np.arange(toks // 32) * 32, np.arange(32), np.arange(n_sp) * toks]
    angles = np.concatenate(parts)[:, None] * np.tile(inverse.astype(np.float64), 4)[None, :]
    turns = np.stack([np.cos(angles), np.sin(angles)]).astype(np.float32)

    n_copies = 2 + 24 + 2 + 2 + 1 + 12 + 4 + 4 * seqs
    vmem = pl.BlockSpec(memory_space=pltpu.VMEM)
    far = pl.BlockSpec(memory_space=pl.ANY)
    call = pl.pallas_call(
        functools.partial(kernel, (seqs, toks, width, xs, zs, ys, tps)),
        out_shape=(
            pltpu.VMEM((seqs, toks // tps, width), BF16),
            pltpu.VMEM((seqs, 2, toks), F32),
        ),
        in_specs=[far] * 9 + [pl.BlockSpec(memory_space=pltpu.SMEM)] + [far] * 3,
        out_specs=(vmem, vmem),
        scratch_shapes=[
            pltpu.VMEM((SLOTS, LN_ROWS, width), BF16),
            pltpu.VMEM((16, width), F32),
            pltpu.VMEM((seqs * toks, width), BF16),
            pltpu.VMEM((zs, xs, 128, 256), BF16),
            pltpu.VMEM((zs, xs, 128, 256), BF16),
            pltpu.VMEM((CORES, 2, zs, xs, ys * 128, 128), BF16),
            pltpu.VMEM((tps, 8, 128), F32),
            pltpu.VMEM((31, 128), F32),
            pltpu.VMEM((128, 128), BF16),
            pltpu.VMEM((width // 128, 128), BF16),
            pltpu.VMEM((31, 128), BF16),
            pltpu.VMEM((1, 128), BF16),
            pltpu.VMEM(turns.shape, F32),
            pltpu.VMEM((toks, 128), F32),
            pltpu.VMEM((toks, 128), F32),
            pltpu.VMEM((seqs, toks + 2 * RIM, 128), F32),
            pltpu.VMEM((seqs, toks // 128, 2, 128, 128), BF16),
            pltpu.VMEM((seqs, toks + 2 * WINDOW, 128), BF16),
            pltpu.VMEM((seqs, HEAD_DIM, toks + 2 * WINDOW), BF16),
            pltpu.VMEM((seqs, 4, WINDOW, 128), BF16),
            pltpu.VMEM((2, WINDOW, 256), F32),
            pltpu.VMEM((2, 3, WINDOW, 256), F32),
            pltpu.VMEM((2, 3, WINDOW, 256), BF16),
            pltpu.VMEM((xs * zs // 2, seqs // 2 * 128, 256), F32),
            pltpu.VMEM((seqs, toks, 128), BF16),
            pltpu.VMEM((seqs, toks, 128), BF16),
            pltpu.VMEM((seqs, toks // tps, tps * 128), BF16),
            pltpu.VMEM((seqs, toks // tps, tps * 256), BF16),
            pltpu.SemaphoreType.DMA((SLOTS,)),
            pltpu.SemaphoreType.DMA((12,)),
            pltpu.SemaphoreType.DMA((n_copies,)),
            pltpu.SemaphoreType.DMA((n_copies,)),
        ],
        compiler_params=pltpu.CompilerParams(
            collective_id=0, has_side_effects=True, vmem_limit_bytes=54 * 2**20
        ),
        name="layer",
    )
    return call(
        tokens,
        norm_gain.reshape(-1, 128),
        conv_value_weight,
        conv_gate_weight,
        query_weight,
        key_weight.T,
        value_weight.T,
        conv_taps,
        conv_gain.reshape(1, -1),
        sink_logit,
        out_conv_weight,
        out_attn_weight,
        jnp.asarray(turns),
    )


def solution(mesh):
    placed = (
        P(None, "sp", None),
        P(),
        P("sp", "tp"),
        P("sp", "tp"),
        P("sp", "tp"),
        P("sp", "tp"),
        P("sp", "tp"),
        P(None, "tp"),
        P("tp"),
        P("tp"),
        P("tp", "sp"),
        P("tp", "sp"),
    )
    xs = int(round(mesh.shape["sp"] ** 0.5))
    shape = (xs, mesh.shape["sp"] // xs, mesh.shape["tp"] // CORES, mesh.shape["tp"])
    return jax.shard_map(
        functools.partial(on_device, shape),
        mesh=mesh,
        in_specs=placed,
        out_specs=(P(None, ("sp", "tp"), None), P(None, "tp", "sp")),
        check_vma=False,
    )
```

```python
import functools
import math

import jax
import jax.numpy as jnp
import numpy as np
from jax import lax
from jax.experimental import pallas as pl
from jax.experimental.pallas import tpu as pltpu
from jax.sharding import PartitionSpec as P

MESH = pl.DeviceIdType.MESH
F32 = jnp.float32
BF16 = jnp.bfloat16

HEAD_DIM = 64
WINDOW = 128
EPSILON = 1e-06
ROPE_BASE = 10000.0
MASK_VALUE = -1e30
RIM = 16
LN_ROWS = 256
CORES = 2
SLOTS = 6


def dot(a, b, dims=((1,), (0,))):
    return lax.dot_general(a, b, (dims, ((), ())), preferred_element_type=F32)


def kernel(
    dims,
    tokens,
    norm_gain,
    w_value,
    w_gate,
    w_query,
    w_key,
    w_val,
    conv_taps,
    conv_gain,
    sink,
    w_oc,
    w_oa,
    turns,
    mixed,
    log_total,
    tbuf,
    gain_buf,
    normed,
    w_a,
    w_b,
    o_w,
    gain_all,
    taps_buf,
    key_buf,
    gain_rows,
    taps_rows,
    conv_gain_row,
    turn_buf,
    cos_ref,
    sin_ref,
    gpad,
    qz,
    kpad,
    val_t,
    edges,
    bias,
    score_buf,
    weight_buf,
    partial_out,
    fsend,
    asend,
    cbm,
    bm,
    tok_sem,
    load_sem,
    send_sem,
    recv_sem,
):
    SEQS, T, D, X, Z, Y, TP = dims
    NSP = X * Z
    per_seq = T // LN_ROWS
    n_blocks = SEQS * per_seq
    sp, tp = lax.axis_index("sp"), lax.axis_index("tp")
    z, x = sp // X, sp % X
    y, c = tp // CORES, tp % CORES
    slot = c * Y + y
    own_rows = pl.ds(pl.multiple_of(y * 128, 128), 128)

    def at_x(d):
        return (z * X + (x + d) % X, tp)

    def at_z(d):
        return (((z + d) % Z) * X + x, tp)

    def at_y(d):
        return (sp, ((y + d) % Y) * CORES + c)

    def at_tp(d):
        return (sp, (tp + d) % TP)

    partner = (sp, y * CORES + (1 - c))
    right = ((sp + 1) % NSP, tp)
    left = ((sp + NSP - 1) % NSP, tp)

    counter = [0]

    def ids(n):
        first = counter[0]
        counter[0] += n
        return first

    def remote(src, dst, i, device, sent=0):
        return pltpu.make_async_remote_copy(
            src_ref=src,
            dst_ref=dst,
            send_sem=send_sem.at[sent],
            recv_sem=recv_sem.at[i],
            device_id=device,
            device_id_type=MESH,
        )

    def start(copies):
        for cp in copies:
            cp.start()

    def group_of(i, pairs, whole, sent=0):
        copies = [remote(src, dst, i, device, sent) for src, dst, device in pairs]
        return copies, remote(whole, whole, i, right, sent), math.prod(whole.shape) * whole.dtype.itemsize

    def arrived(group):
        group[1].wait_recv()

    class Ring:
        def __init__(self, part, whole, me, size, at):
            i = ids(6)
            before, after = (me + size - 1) % size, (me + 1) % size

            def half(n, k, h, d):
                return group_of(i + n, [(ref, ref, at(d)) for ref in part(k, h)], whole)

            self.direct = [half(0, me, 0, 1)]
            self.relayed, self.late = [], [half(1, me, 1, 1)]
            self.passed, self.rest = [], []
            if size == 2:
                return
            self.direct.append(half(2, me, 1, size - 1))
            self.late.append(half(3, me, 0, size - 1))
            self.relayed = [half(4, before, 0, 1), half(5, after, 1, size - 1)]
            self.passed = part(before, 0) + part(after, 1)
            self.rest = part(before, 1) + part(after, 0)

        def begin(self):
            self.begin_direct()
            self.begin_late()

        def begin_direct(self):
            for group in self.direct:
                start(group[0])

        def begin_late(self):
            for group in self.late:
                start(group[0])

        def relay(self):
            for group in self.direct:
                arrived(group)
            for group in self.relayed:
                start(group[0])

        def near(self):
            for group in self.late:
                arrived(group)

        def finish(self):
            for group in self.relayed:
                arrived(group)

        def groups(self):
            return self.direct + self.late + self.relayed

    def tok_copy(i):
        seq, r = i // per_seq, (i % per_seq) * LN_ROWS
        return pltpu.make_async_copy(
            tokens.at[seq, pl.ds(pl.multiple_of(r, LN_ROWS), LN_ROWS)],
            tbuf.at[i % SLOTS],
            tok_sem.at[i % SLOTS],
        )

    barrier = pltpu.get_barrier_semaphore()
    greeted = (
        [at_x(d) for d in range(1, X)]
        + [at_z(d) for d in range(1, Z)]
        + [left, right]
        + [at_tp(d) for d in range(1, TP)]
    )
    for device in greeted:
        pl.semaphore_signal(barrier, inc=1, device_id=device, device_id_type=MESH)

    wanted = [
        (w_value, w_a.at[z, x, :, pl.ds(0, 128)]),
        (w_gate, w_a.at[z, x, :, pl.ds(128, 128)]),
        (w_query, w_b.at[z, x, :, pl.ds(0, 128)]),
        (w_oc, o_w.at[c, 0, z, x, own_rows]),
        (w_oa, o_w.at[c, 1, z, x, own_rows]),
        (w_key, key_buf.at[pl.ds(0, 64)]),
        (w_val, key_buf.at[pl.ds(64, 64)]),
        (conv_taps, taps_rows),
        (turns.at[0], turn_buf.at[0]),
        (turns.at[1], turn_buf.at[1]),
        (norm_gain, gain_rows),
        (conv_gain, conv_gain_row),
    ]
    loads = [pltpu.make_async_copy(a, b, load_sem.at[n]) for n, (a, b) in enumerate(wanted)]
    for n in (5, 6, 8, 9, 0, 1, 2, 3, 4, 7, 10, 11):
        loads[n].start()

    for n in range(SLOTS - 1):
        tok_copy(n).start()

    half_x, half_z = X // 2, Z // 2

    def others(block, me, size, h):
        if size == 2:
            return [block(1 - me).at[pl.ds(h * 32, 32)]]
        opposite = block((me + 2) % size).at[pl.ds(h * 32, 32)]
        return [block((me + 1 + 2 * h) % size), opposite]

    def gather_of(w):
        mine = [w.at[z, x, pl.ds(64 * f, 64)] for f in range(2)]
        first = [
            group_of(ids(1), [(mine[0], mine[0], at_x(d)) for d in range(1, X)], w.at[0, pl.ds(0, X - 1), pl.ds(0, 64)]),
            group_of(ids(1), [(mine[1], mine[1], at_z(d)) for d in range(1, Z)], w.at[pl.ds(0, Z - 1), 0, pl.ds(0, 64)]),
        ]
        own = [
            Ring(lambda k, h: [w.at[k, x, pl.ds(h * 32, 32)]], w.at[0, 0, pl.ds(0, 32)], z, Z, at_z),
            Ring(lambda k, h: [w.at[z, k, pl.ds(64 + h * 32, 32)]], w.at[0, 0, pl.ds(0, 32)], x, X, at_x),
        ]
        most = w.at[0, pl.ds(0, X - 1), pl.ds(0, 32)]
        rest = [
            Ring(lambda k, h: others(lambda n: w.at[k, n, pl.ds(0, 64)], x, X, h), most, z, Z, at_z),
            Ring(lambda k, h: others(lambda n: w.at[n, k, pl.ds(64, 64)], z, Z, h), most, x, X, at_x),
        ]
        return first, own, rest

    first_a, own_a, rest_a = gather_of(w_a)
    first_b, own_b, rest_b = gather_of(w_b)
    own_gain = gain_all.at[slot]
    gains = group_of(ids(1), [(own_gain, own_gain, at_tp(d)) for d in range(1, TP)], gain_all.at[pl.ds(0, TP - 1)], 1)
    tile_0, tile_1 = o_w.at[c, 0, z, x, own_rows], o_w.at[c, 1, z, x, own_rows]
    out_0 = [
        group_of(ids(1), [(tile_0, tile_0, at_x(d)) for d in range(1, X)], fsend.at[0, pl.ds(0, (X - 1) * 128)]),
        group_of(ids(1), [(tile_1, tile_1, at_z(d)) for d in range(1, Z)], fsend.at[0, pl.ds(0, (Z - 1) * 128)]),
    ]
    def rows_from(k):
        return pl.ds(pl.multiple_of(k * 128, 128), 128)

    quarter = o_w.at[0, 0, 0, pl.ds(0, half_x), pl.ds(0, 128)]
    out_1 = [
        Ring(lambda k, h: [o_w.at[c, 0, z, pl.ds(h * half_x, half_x), rows_from(k)]], quarter, y, Y, at_y),
        Ring(lambda k, h: [o_w.at[c, 1, pl.ds(h * half_z, half_z), x, rows_from(k)]], quarter, y, Y, at_y),
    ]
    out_2 = [
        Ring(lambda k, h: [o_w.at[c, 0, k, pl.ds(h * half_x, half_x)]], o_w.at[0, 0, 0, pl.ds(0, half_x)], z, Z, at_z),
        Ring(lambda k, h: [o_w.at[c, 1, pl.ds(h * half_z, half_z), k]], o_w.at[0, 0, 0, pl.ds(0, half_x)], x, X, at_x),
    ]

    def to_partner(d):
        row, column = o_w.at[c, 0, (z + d) % Z], o_w.at[c, 1, :, (x + d) % X]
        return [(row, row, partner), (column, column, partner)]

    pair_1 = group_of(ids(1), to_partner(0), o_w.at[0, 0, pl.ds(0, 2)])
    pairs = [pair_1]
    if X == 2:
        pair_4 = group_of(ids(1), to_partner(1), o_w.at[0, 0, pl.ds(0, 2)])
        pairs += [pair_4]
    else:
        passed = [(ref, ref, partner) for ring in out_2 for ref in ring.passed]
        rest = [(ref, ref, partner) for ring in out_2 for ref in ring.rest]
        pair_2 = group_of(ids(1), passed, o_w.at[0, 0, pl.ds(0, 2)])
        pair_3 = group_of(ids(1), rest, o_w.at[0, 0, pl.ds(0, 2)])
        pair_4 = group_of(ids(1), to_partner(2), o_w.at[0, 0, pl.ds(0, 2)])
        pairs += [pair_2, pair_3, pair_4]

    rim_i, keys_i = ids(SEQS), ids(SEQS)

    def rims(s):
        return group_of(
            rim_i + s,
            [
                (gpad.at[s, pl.ds(RIM, RIM)], gpad.at[s, pl.ds(RIM + T, RIM)], left),
                (gpad.at[s, pl.ds(T, RIM)], gpad.at[s, pl.ds(0, RIM)], right),
            ],
            gpad.at[0, pl.ds(0, 2 * RIM)],
        )

    def edge_keys(s):
        return group_of(
            keys_i + s,
            [(edges.at[s, 1], edges.at[s, 3], left), (edges.at[s, 2], edges.at[s, 0], right)],
            edges.at[0, pl.ds(0, 2)],
        )

    conv_i, attn_i = ids(SEQS), ids(SEQS)
    peers_rows = fsend.at[0, pl.ds(0, (TP - 1) * 128)]

    def rows_of(device_tp):
        return pl.ds(pl.multiple_of(device_tp * 128, 128), 128)

    conv_lanes = pl.ds(pl.multiple_of(slot * 128, 128), 128)
    attn_lanes = pl.ds(pl.multiple_of(c * (Y * 256) + (Y + y) * 128, 128), 128)

    def conv_out_copies(s):
        return group_of(
            conv_i + s,
            [
                (fsend.at[s, rows_of((tp + d) % TP)], cbm.at[s, :, conv_lanes], at_tp(d))
                for d in range(1, TP)
            ],
            peers_rows,
        )

    def attn_out_copies(s):
        return group_of(
            attn_i + s,
            [
                (asend.at[s, rows_of((tp + d) % TP)], bm.at[s, :, attn_lanes], at_tp(d))
                for d in range(1, TP)
            ],
            peers_rows,
        )

    for n in range(2):
        loads[n].wait()
    with jax.named_scope("greet"):
        pl.semaphore_wait(barrier, len(greeted))
    for group in first_a:
        start(group[0])
    for ring in own_a:
        ring.begin()

    for n in (8, 9, 10):
        loads[n].wait()
    run = turn_buf.shape[1] - NSP - 32
    cos_s, sin_s = turn_buf[0, pl.ds(run + 32 + sp, 1), :], turn_buf[1, pl.ds(run + 32 + sp, 1), :]
    cos_b, sin_b = turn_buf[0, run : run + 32, :], turn_buf[1, run : run + 32, :]
    cos_bs, sin_bs = cos_b * cos_s - sin_b * sin_s, sin_b * cos_s + cos_b * sin_s
    low_half = (lax.broadcasted_iota(jnp.int32, (1, 128), 1) % HEAD_DIM) < HEAD_DIM // 2
    sign = jnp.where(low_half, -1.0, 1.0)

    def turn(n, carry):
        cos_a, sin_a = turn_buf[0, pl.ds(n, 1), :], turn_buf[1, pl.ds(n, 1), :]
        at = pl.ds(pl.multiple_of(n * 32, 32), 32)
        cos_ref[at, :] = cos_bs * cos_a - sin_bs * sin_a
        sin_ref[at, :] = (sin_bs * cos_a + cos_bs * sin_a) * sign
        return carry

    lax.fori_loop(0, T // 32, turn, 0, unroll=2)

    for n in (5, 6, 7):
        loads[n].wait()
    w_b[z, x, :, 128:256] = key_buf[...].astype(F32).T.astype(BF16)
    taps_buf[...] = taps_rows[...].astype(F32)
    for n in range(D // 128):
        gain_buf[:, n * 128 : (n + 1) * 128] = jnp.broadcast_to(
            gain_rows[n : n + 1, :].astype(F32), (16, 128)
        )
    loads[11].wait()
    gain_all[slot] = jnp.broadcast_to(conv_gain_row[...].astype(F32), (8, 128))
    key_i = lax.broadcasted_iota(jnp.int32, (WINDOW, 256), 0)
    query_i = lax.broadcasted_iota(jnp.int32, (WINDOW, 256), 1) % WINDOW
    bias[0] = jnp.where(key_i >= query_i, 0.0, MASK_VALUE)
    bias[1] = jnp.where(key_i <= query_i, 0.0, MASK_VALUE)
    for n in range(2, 5):
        loads[n].wait()

    def ln_block(i, carry):
        tok_copy(i).wait()

        @pl.when(i + SLOTS - 1 < n_blocks)
        def _():
            tok_copy(i + SLOTS - 1).start()

        def group(g, carry):
            at = pl.ds(pl.multiple_of(i * LN_ROWS, LN_ROWS) + pl.multiple_of(g * 16, 16), 16)
            v = tbuf[i % SLOTS, pl.ds(pl.multiple_of(g * 16, 16), 16), :].astype(F32)
            mean = jnp.sum(v, axis=-1, keepdims=True) * (1.0 / D)
            centred = v - mean
            var = jnp.sum(centred * centred, axis=-1, keepdims=True) * (1.0 / D)
            out = centred * lax.rsqrt(var + EPSILON) * gain_buf[...]
            normed[at, :] = out.astype(BF16)
            return carry

        return lax.fori_loop(0, LN_ROWS // 16, group, carry, unroll=16)

    def norm_blocks(first, last):
        with jax.named_scope("norm"):
            lax.fori_loop(n_blocks * first // 16, n_blocks * last // 16, ln_block, 0)

    norm_blocks(0, 2)
    for group in first_b + out_0 + [gains]:
        start(group[0])
    norm_blocks(2, 5)
    with jax.named_scope("wait_in_1"):
        for group in first_a:
            arrived(group)
    for ring in rest_a:
        ring.begin()
    with jax.named_scope("wait_own"):
        for ring in own_a:
            ring.relay()
    for ring in own_b:
        ring.begin()
    norm_blocks(5, 7)
    with jax.named_scope("wait_in_b1"):
        for group in first_b:
            arrived(group)
    for ring in rest_b:
        ring.begin()
    norm_blocks(7, 9)
    with jax.named_scope("wait_out_0"):
        for group in out_0:
            arrived(group)
    for ring in out_1:
        ring.begin_direct()
    for ring in out_1:
        ring.begin_late()
    norm_blocks(9, 11)
    with jax.named_scope("wait_relay"):
        for ring in rest_a + own_b:
            ring.relay()
    norm_blocks(11, 16)
    with jax.named_scope("wait_relay_b"):
        for ring in rest_b + out_1:
            ring.relay()
    with jax.named_scope("wait_in_a"):
        for ring in own_a + rest_a:
            ring.near()
            ring.finish()

    lane = lax.broadcasted_iota(jnp.int32, (1, 128), 1)
    low_head = lane < HEAD_DIM

    def swapped(v):
        return jnp.where(low_half, pltpu.roll(v, 96, 1), pltpu.roll(v, 32, 1))

    def gate(s, starts):
        n = 256 // len(starts)
        at = [pl.ds(pl.multiple_of(s * T + r, 128), n) for r in starts]
        rows = jnp.concatenate([normed[rs, :] for rs in at], axis=0)
        a = dot(rows, w_a[...].reshape(D, 256))
        gated = a[:, :128] * jax.nn.sigmoid(a[:, 128:])
        gated = gated.astype(BF16).astype(F32)
        for k in range(2):
            r = pl.multiple_of(starts[k] if len(starts) == 2 else starts[0] + k * 128, 128)
            gpad[s, pl.ds(RIM + r, 128), :] = gated[k * 128 : (k + 1) * 128]

    def project(s, starts):
        n = 256 // len(starts)
        at = [pl.ds(pl.multiple_of(s * T + r, 128), n) for r in starts]
        rows = jnp.concatenate([normed[rs, :] for rs in at], axis=0)
        b = dot(rows, w_b[...].reshape(D, 256))
        at = [pl.ds(pl.multiple_of(r, 128), n) for r in starts]
        cosine = jnp.concatenate([cos_ref[rs, :] for rs in at], axis=0)
        sine = jnp.concatenate([sin_ref[rs, :] for rs in at], axis=0)
        q, kv = b[:, :128], b[:, 128:]
        q = (q * cosine + swapped(q) * sine) * (HEAD_DIM**-0.5)
        zero = jnp.zeros_like(q)
        q_0 = jnp.where(low_head, q, zero).astype(BF16)
        q_1 = jnp.where(low_head, zero, q).astype(BF16)
        turned = kv * cosine + swapped(kv) * sine
        twice = jnp.where(low_head, turned, pltpu.roll(turned, 64, 1)).astype(BF16)
        kv = jnp.where(low_head, turned, kv).astype(BF16)
        for k in range(2):
            r = pl.multiple_of(starts[k] if len(starts) == 2 else starts[0] + k * 128, 128)
            part = slice(k * 128, (k + 1) * 128)
            qz[s, r // 128, 0] = q_0[part]
            qz[s, r // 128, 1] = q_1[part]
            kpad[s, pl.ds(WINDOW + r, 128), :] = twice[part]
            val_t[s, :, pl.ds(WINDOW + r, 128)] = kv[part].T[64:]
            if len(starts) == 2:
                edges[s, k + 1] = kv[part]

    def convolve(s):
        with jax.named_scope("wait_rim"):
            arrived(rims(s))

        @pl.when(sp == 0)
        def _():
            gpad[s, pl.ds(0, RIM), :] = jnp.zeros((RIM, 128), F32)

        @pl.when(sp == NSP - 1)
        def _():
            gpad[s, pl.ds(RIM + T, RIM), :] = jnp.zeros((RIM, 128), F32)

        def chunk(k, carry):
            r = pl.multiple_of(k * 128, 128)
            total = jnp.zeros((128, 128), F32)
            for j in range(31):
                total = total + gpad[s, pl.ds(r + (j + 1), 128), :] * taps_buf[pl.ds(j, 1), :]
            fsend[s, pl.ds(r, 128), :] = total.astype(BF16)
            return carry

        with jax.named_scope("conv"):
            lax.fori_loop(0, T // 128, chunk, 0)
        start(conv_out_copies(s)[0])
        cbm[s, :, conv_lanes] = fsend[s, rows_of(tp), :]

    def gate_edges(k, carry):
        for s in (2 * k, 2 * k + 1):
            gate(s, (0, T - 128))
        for s in (2 * k, 2 * k + 1):
            start(rims(s)[0])
        return carry

    def project_edges(k, carry):
        for s in (2 * k, 2 * k + 1):
            project(s, (0, T - 128))
        for s in (2 * k, 2 * k + 1):
            start(edge_keys(s)[0])
        return carry

    inner = T // 256 - 1

    def inner_rows(s, step):
        lax.fori_loop(0, inner, lambda k, carry: step(s, (128 + k * 256,)) or carry, 0, unroll=inner)

    def gate_inner(s, carry):
        inner_rows(s, gate)
        return carry

    def each_convolve(s, carry):
        convolve(s)
        return carry

    with jax.named_scope("gate_edges"):
        lax.fori_loop(0, SEQS // 2, gate_edges, 0)
    with jax.named_scope("gate_inner"):
        lax.fori_loop(0, SEQS, gate_inner, 0)
    with jax.named_scope("wait_out_1"):
        for ring in out_1:
            ring.near()
            ring.finish()
    for ring in out_2:
        ring.begin_direct()
    with jax.named_scope("wait_in_b"):
        for ring in own_b + rest_b:
            ring.near()
            ring.finish()
    with jax.named_scope("project_edges"):
        lax.fori_loop(0, SEQS // 2, project_edges, 0)
    for ring in out_2:
        ring.begin_late()
    start(pair_1[0])
    lax.fori_loop(0, SEQS, each_convolve, 0)

    head_lane = lax.broadcasted_iota(jnp.int32, (1, 256), 1)
    sink_row = jnp.where(head_lane < 128, sink[0], sink[1])

    def widen(s, e, first):
        kv = edges[s, e].astype(F32)
        kpad[s, pl.ds(first, WINDOW), :] = jnp.where(low_head, kv, pltpu.roll(kv, 64, 1)).astype(BF16)
        val_t[s, :, pl.ds(first, WINDOW)] = edges[s, e].T[64:]

    blocks = T // 128

    def attend(s):
        with jax.named_scope("wait_keys"):
            arrived(edge_keys(s))
        widen(s, 0, 0)
        widen(s, 3, WINDOW + T)

        tops, totals = {}, {}

        def score(b):
            keys = kpad[s, pl.ds(b * 128, 384), :]
            scores = dot(keys, qz[s, b].reshape(256, 128), ((1,), (1,)))
            low, high = bias[0], bias[1]
            if b == 0:
                low = low + jnp.where(sp == 0, MASK_VALUE, 0.0)
            if b == blocks - 1:
                high = high + jnp.where(sp == NSP - 1, MASK_VALUE, 0.0)
            s_0, s_1, s_2 = scores[:128] + low, scores[128:256], scores[256:] + high
            top = jnp.max(jnp.maximum(jnp.maximum(s_0, s_1), s_2), axis=0, keepdims=True)
            tops[b] = jnp.maximum(top, sink_row)
            for n, part in enumerate((s_0, s_1, s_2)):
                score_buf[b % 2, n] = part

        def weigh(b):
            top = tops[b]
            e_0, e_1, e_2 = (jnp.exp(score_buf[b % 2, n] - top) for n in range(3))
            total = jnp.sum(e_0 + e_1 + e_2, axis=0, keepdims=True) + jnp.exp(sink_row - top)
            totals[b] = total
            logs = top + jnp.log(total)
            log_total[s, :, pl.ds(b * 128, 128)] = jnp.concatenate([logs[:, :128], logs[:, 128:]], axis=0)
            for n, part in enumerate((e_0, e_1, e_2)):
                weight_buf[b % 2, n] = part.astype(BF16)

        def collect(b):
            weights = weight_buf[b % 2].reshape(384, 256)
            out = dot(val_t[s, :, pl.ds(b * 128, 384)], weights) * (1.0 / totals[b])
            both = jnp.concatenate([out[:, :128], out[:, 128:]], axis=0)
            asend[s, pl.ds(b * 128, 128), :] = both.astype(BF16).T

        with jax.named_scope("attend"):
            for b in range(blocks + 2):
                if b < blocks:
                    score(b)
                if 0 <= b - 1 < blocks:
                    weigh(b - 1)
                if b >= 2:
                    collect(b - 2)
        start(attn_out_copies(s)[0])
        bm[s, :, attn_lanes] = asend[s, rows_of(tp), :]

    def sequence(s, carry):
        @pl.when(s == SEQS - 1)
        def _():
            with jax.named_scope("wait_out_near"):
                for ring in out_2:
                    ring.near()
            if X > 2:
                start(pair_3[0])

        with jax.named_scope("project"):
            inner_rows(s, project)

        @pl.when(s == 0)
        def _():
            with jax.named_scope("wait_out_relay"):
                for ring in out_2:
                    ring.relay()
            if X > 2:
                start(pair_2[0])

        attend(s)
        return carry

    lax.fori_loop(0, SEQS, sequence, 0)
    arrived(gains)

    def finish(s):
        with jax.named_scope("wait_conv"):
            arrived(conv_out_copies(s))

        def group(g, carry):
            at = pl.ds(pl.multiple_of(g * 16, 16), 16)
            v = cbm[s, at, :].astype(F32)
            mean = jnp.sum(v, axis=-1, keepdims=True) * (1.0 / (TP * 128))
            centred = v - mean
            var = jnp.sum(centred * centred, axis=-1, keepdims=True) * (1.0 / (TP * 128))
            scale = lax.rsqrt(var + EPSILON)
            for n in range(TP):
                u = centred[:, n * 128 : (n + 1) * 128] * scale * gain_all[n, 0:1, :]
                first = n // Y * (Y * 256) + n % Y * 128
                bm[s, at, first : first + 128] = jax.nn.silu(u).astype(BF16)
            return carry

        with jax.named_scope("channel_norm"):
            lax.fori_loop(0, 128 // 16, group, 0, unroll=8)

    def out_pair(blocks, h):
        at = [((z + dz) % Z, (x + dx) % X) for dz, dx in blocks]
        pieces = [
            jnp.concatenate([o_w[cc, hh, zz, xx] for zz, xx in at], axis=1)
            for cc in range(CORES)
            for hh in h
        ]
        columns = [pl.ds(pl.multiple_of((zz * X + xx) * 128, 128), 128) for zz, xx in at]
        return jnp.concatenate(pieces, axis=0), columns

    everything = [(dz, dx) for dz in range(Z) for dx in range(X)]
    early = [k for k in everything if X > 2 and 2 not in k]
    early = early[: len(early) // 2 * 2]
    late = [k for k in everything if k not in early]
    early, late = ([b[n : n + 2] for n in range(0, len(b), 2)] for b in (early, late))
    branch = Y * 128
    half = SEQS // 2

    def rows_out(seqs, h):
        first = [(2 * cc + h) * branch for cc in range(CORES)]
        n = seqs.stop - seqs.start
        lanes = [bm[seqs, :, k : k + branch].reshape(n * 128, branch) for k in first]
        return jnp.concatenate(lanes, axis=1)

    def out_conv(n, blocks):
        acc = dot(rows_out(slice(0, SEQS), 0), out_pair(blocks, (0,))[0])
        partial_out[n] = acc.reshape(SEQS, 128, 256)

    def out_attn(n, blocks, seqs):
        weights, columns = out_pair(blocks, (1,))
        count = seqs.stop - seqs.start
        acc = dot(rows_out(seqs, 1), weights).reshape(count, 128, 256) + partial_out[n, seqs]
        acc = acc.astype(BF16)
        for n in range(2):
            mixed[seqs, :, columns[n]] = acc[:, :, n * 128 : (n + 1) * 128]

    early = list(enumerate(early))
    late = [(len(early) + n, blocks) for n, blocks in enumerate(late)]
    for s in range(SEQS):
        finish(s)
    with jax.named_scope("wait_pair"):
        for group in pairs[:-1]:
            arrived(group)
    with jax.named_scope("out_conv"):
        for n, blocks in early:
            out_conv(n, blocks)
    with jax.named_scope("wait_out_2"):
        for ring in out_2:
            ring.finish()
    start(pair_4[0])
    with jax.named_scope("wait_attn"):
        for s in range(half):
            arrived(attn_out_copies(s))
    with jax.named_scope("out_attn"):
        for n, blocks in early:
            out_attn(n, blocks, slice(0, half))
    with jax.named_scope("wait_pair"):
        arrived(pair_4)
    with jax.named_scope("out_conv"):
        for n, blocks in late:
            out_conv(n, blocks)
    with jax.named_scope("out_attn"):
        for n, blocks in late:
            out_attn(n, blocks, slice(0, half))
    with jax.named_scope("wait_attn"):
        for s in range(half, SEQS):
            arrived(attn_out_copies(s))
    with jax.named_scope("out_attn"):
        for n, blocks in early + late:
            out_attn(n, blocks, slice(half, SEQS))

    rings = own_a + rest_a + own_b + rest_b + out_1 + out_2
    groups = first_a + first_b + out_0 + pairs + [group for ring in rings for group in ring.groups()]
    for s in range(SEQS):
        groups += [rims(s), edge_keys(s), conv_out_copies(s), attn_out_copies(s)]
    sent_rows = sum(group[2] for group in groups) // (2 * D)
    gains[1].wait_send()
    while sent_rows > 0:
        gone = normed.at[pl.ds(0, min(sent_rows, SEQS * T))]
        remote(gone, gone, 0, right).wait_send()
        sent_rows -= SEQS * T


def on_device(
    grid_shape,
    tokens,
    norm_gain,
    conv_value_weight,
    conv_gate_weight,
    query_weight,
    key_weight,
    value_weight,
    conv_taps,
    conv_gain,
    sink_logit,
    out_conv_weight,
    out_attn_weight,
):
    seqs, toks, width = tokens.shape
    xs, zs, ys, tps = grid_shape
    n_sp = xs * zs
    half = HEAD_DIM // 2
    inverse = (ROPE_BASE ** (-np.arange(half, dtype=np.float32) / half)).astype(np.float32)
    parts = [np.arange(toks // 32) * 32, np.arange(32), np.arange(n_sp) * toks]
    angles = np.concatenate(parts)[:, None] * np.tile(inverse.astype(np.float64), 4)[None, :]
    turns = np.stack([np.cos(angles), np.sin(angles)]).astype(np.float32)

    n_copies = 4 + 48 + 2 + 12 + 1 + 12 + 4 + 4 * seqs
    vmem = pl.BlockSpec(memory_space=pltpu.VMEM)
    far = pl.BlockSpec(memory_space=pl.ANY)
    call = pl.pallas_call(
        functools.partial(kernel, (seqs, toks, width, xs, zs, ys, tps)),
        out_shape=(
            pltpu.VMEM((seqs, toks // tps, width), BF16),
            pltpu.VMEM((seqs, 2, toks), F32),
        ),
        in_specs=[far] * 9 + [pl.BlockSpec(memory_space=pltpu.SMEM)] + [far] * 3,
        out_specs=(vmem, vmem),
        scratch_shapes=[
            pltpu.VMEM((SLOTS, LN_ROWS, width), BF16),
            pltpu.VMEM((16, width), F32),
            pltpu.VMEM((seqs * toks, width), BF16),
            pltpu.VMEM((zs, xs, 128, 256), BF16),
            pltpu.VMEM((zs, xs, 128, 256), BF16),
            pltpu.VMEM((CORES, 2, zs, xs, ys * 128, 128), BF16),
            pltpu.VMEM((tps, 8, 128), F32),
            pltpu.VMEM((31, 128), F32),
            pltpu.VMEM((128, 128), BF16),
            pltpu.VMEM((width // 128, 128), BF16),
            pltpu.VMEM((31, 128), BF16),
            pltpu.VMEM((1, 128), BF16),
            pltpu.VMEM(turns.shape, F32),
            pltpu.VMEM((toks, 128), F32),
            pltpu.VMEM((toks, 128), F32),
            pltpu.VMEM((seqs, toks + 2 * RIM, 128), F32),
            pltpu.VMEM((seqs, toks // 128, 2, 128, 128), BF16),
            pltpu.VMEM((seqs, toks + 2 * WINDOW, 128), BF16),
            pltpu.VMEM((seqs, HEAD_DIM, toks + 2 * WINDOW), BF16),
            pltpu.VMEM((seqs, 4, WINDOW, 128), BF16),
            pltpu.VMEM((2, WINDOW, 256), F32),
            pltpu.VMEM((2, 3, WINDOW, 256), F32),
            pltpu.VMEM((2, 3, WINDOW, 256), BF16),
            pltpu.VMEM((xs * zs // 2, seqs, 128, 256), F32),
            pltpu.VMEM((seqs, toks, 128), BF16),
            pltpu.VMEM((seqs, toks, 128), BF16),
            pltpu.VMEM((seqs, toks // tps, tps * 128), BF16),
            pltpu.VMEM((seqs, toks // tps, tps * 256), BF16),
            pltpu.SemaphoreType.DMA((SLOTS,)),
            pltpu.SemaphoreType.DMA((12,)),
            pltpu.SemaphoreType.DMA((2,)),
            pltpu.SemaphoreType.DMA((n_copies,)),
        ],
        compiler_params=pltpu.CompilerParams(
            collective_id=0, has_side_effects=True, vmem_limit_bytes=54 * 2**20
        ),
        name="layer",
    )
    return call(
        tokens,
        norm_gain.reshape(-1, 128),
        conv_value_weight,
        conv_gate_weight,
        query_weight,
        key_weight.T,
        value_weight.T,
        conv_taps,
        conv_gain.reshape(1, -1),
        sink_logit,
        out_conv_weight,
        out_attn_weight,
        jnp.asarray(turns),
    )


def solution(mesh):
    placed = (
        P(None, "sp", None),
        P(),
        P("sp", "tp"),
        P("sp", "tp"),
        P("sp", "tp"),
        P("sp", "tp"),
        P("sp", "tp"),
        P(None, "tp"),
        P("tp"),
        P("tp"),
        P("tp", "sp"),
        P("tp", "sp"),
    )
    xs = int(round(mesh.shape["sp"] ** 0.5))
    shape = (xs, mesh.shape["sp"] // xs, mesh.shape["tp"] // CORES, mesh.shape["tp"])
    return jax.shard_map(
        functools.partial(on_device, shape),
        mesh=mesh,
        in_specs=placed,
        out_specs=(P(None, ("sp", "tp"), None), P(None, "tp", "sp")),
        check_vma=False,
    )
```

```python
import functools
import math

import jax
import jax.numpy as jnp
import numpy as np
from jax import lax
from jax.experimental import pallas as pl
from jax.experimental.pallas import tpu as pltpu
from jax.sharding import PartitionSpec as P

MESH = pl.DeviceIdType.MESH
F32 = jnp.float32
BF16 = jnp.bfloat16

HEAD_DIM = 64
WINDOW = 128
EPSILON = 1e-06
ROPE_BASE = 10000.0
MASK_VALUE = -1e30
RIM = 16
LN_ROWS = 256
CORES = 2
SLOTS = 6


def dot(a, b, dims=((1,), (0,))):
    return lax.dot_general(a, b, (dims, ((), ())), preferred_element_type=F32)


def kernel(
    dims,
    tokens,
    norm_gain,
    w_value,
    w_gate,
    w_query,
    w_key,
    w_val,
    conv_taps,
    conv_gain,
    sink,
    w_oc,
    w_oa,
    turns,
    mixed,
    log_total,
    tbuf,
    gain_buf,
    normed,
    w_a,
    w_b,
    o_w,
    gain_all,
    taps_buf,
    key_buf,
    gain_rows,
    taps_rows,
    conv_gain_row,
    turn_buf,
    cos_ref,
    sin_ref,
    gpad,
    qz,
    kpad,
    val_t,
    edges,
    bias,
    score_buf,
    weight_buf,
    partial_out,
    fsend,
    asend,
    cbm,
    bm,
    tok_sem,
    load_sem,
    send_sem,
    recv_sem,
):
    SEQS, T, D, X, Z, Y, TP = dims
    NSP = X * Z
    per_seq = T // LN_ROWS
    n_blocks = SEQS * per_seq
    sp, tp = lax.axis_index("sp"), lax.axis_index("tp")
    z, x = sp // X, sp % X
    y, c = tp // CORES, tp % CORES
    slot = c * Y + y
    own_rows = pl.ds(pl.multiple_of(y * 128, 128), 128)

    def at_x(d):
        return (z * X + (x + d) % X, tp)

    def at_z(d):
        return (((z + d) % Z) * X + x, tp)

    def at_y(d):
        return (sp, ((y + d) % Y) * CORES + c)

    def at_tp(d):
        return (sp, (tp + d) % TP)

    partner = (sp, y * CORES + (1 - c))
    right = ((sp + 1) % NSP, tp)
    left = ((sp + NSP - 1) % NSP, tp)

    counter = [0]

    def ids(n):
        first = counter[0]
        counter[0] += n
        return first

    def remote(src, dst, i, device, sent=0):
        return pltpu.make_async_remote_copy(
            src_ref=src,
            dst_ref=dst,
            send_sem=send_sem.at[sent],
            recv_sem=recv_sem.at[i],
            device_id=device,
            device_id_type=MESH,
        )

    def start(copies):
        for cp in copies:
            cp.start()

    def group_of(i, pairs, whole, sent=0):
        copies = [remote(src, dst, i, device, sent) for src, dst, device in pairs]
        return copies, remote(whole, whole, i, right, sent), math.prod(whole.shape) * whole.dtype.itemsize

    def arrived(group):
        group[1].wait_recv()

    class Ring:
        def __init__(self, part, whole, me, size, at):
            i = ids(6)
            before, after = (me + size - 1) % size, (me + 1) % size

            def half(n, k, h, d):
                return group_of(i + n, [(ref, ref, at(d)) for ref in part(k, h)], whole)

            self.direct = [half(0, me, 0, 1)]
            self.relayed, self.late = [], [half(1, me, 1, 1)]
            self.passed, self.rest = [], []
            if size == 2:
                return
            self.direct.append(half(2, me, 1, size - 1))
            self.late.append(half(3, me, 0, size - 1))
            self.relayed = [half(4, before, 0, 1), half(5, after, 1, size - 1)]
            self.passed = part(before, 0) + part(after, 1)
            self.rest = part(before, 1) + part(after, 0)

        def begin(self):
            self.begin_direct()
            self.begin_late()

        def begin_direct(self):
            for group in self.direct:
                start(group[0])

        def begin_late(self):
            for group in self.late:
                start(group[0])

        def relay(self):
            for group in self.direct:
                arrived(group)
            for group in self.relayed:
                start(group[0])

        def near(self):
            for group in self.late:
                arrived(group)

        def finish(self):
            for group in self.relayed:
                arrived(group)

        def groups(self):
            return self.direct + self.late + self.relayed

    def tok_copy(i):
        seq, r = i // per_seq, (i % per_seq) * LN_ROWS
        return pltpu.make_async_copy(
            tokens.at[seq, pl.ds(pl.multiple_of(r, LN_ROWS), LN_ROWS)],
            tbuf.at[i % SLOTS],
            tok_sem.at[i % SLOTS],
        )

    barrier = pltpu.get_barrier_semaphore()
    greeted = (
        [at_x(d) for d in range(1, X)]
        + [at_z(d) for d in range(1, Z)]
        + [left, right]
        + [at_tp(d) for d in range(1, TP)]
    )
    for device in greeted:
        pl.semaphore_signal(barrier, inc=1, device_id=device, device_id_type=MESH)

    wanted = [
        (w_value, w_a.at[z, x, :, pl.ds(0, 128)]),
        (w_gate, w_a.at[z, x, :, pl.ds(128, 128)]),
        (w_query, w_b.at[z, x, :, pl.ds(0, 128)]),
        (w_oc, o_w.at[c, 0, z, x, own_rows]),
        (w_oa, o_w.at[c, 1, z, x, own_rows]),
        (w_key, key_buf.at[pl.ds(0, 64)]),
        (w_val, key_buf.at[pl.ds(64, 64)]),
        (conv_taps, taps_rows),
        (turns.at[0], turn_buf.at[0]),
        (turns.at[1], turn_buf.at[1]),
        (norm_gain, gain_rows),
        (conv_gain, conv_gain_row),
    ]
    loads = [pltpu.make_async_copy(a, b, load_sem.at[n]) for n, (a, b) in enumerate(wanted)]
    for n in (5, 6, 8, 9, 0, 1, 2, 3, 4, 7, 10, 11):
        loads[n].start()

    for n in range(SLOTS - 1):
        tok_copy(n).start()

    half_x, half_z = X // 2, Z // 2

    def others(block, me, size, h):
        if size == 2:
            return [block(1 - me).at[pl.ds(h * 32, 32)]]
        opposite = block((me + 2) % size).at[pl.ds(h * 32, 32)]
        return [block((me + 1 + 2 * h) % size), opposite]

    def gather_of(w):
        mine = [w.at[z, x, pl.ds(64 * f, 64)] for f in range(2)]
        first = [
            group_of(ids(1), [(mine[0], mine[0], at_x(d)) for d in range(1, X)], w.at[0, pl.ds(0, X - 1), pl.ds(0, 64)]),
            group_of(ids(1), [(mine[1], mine[1], at_z(d)) for d in range(1, Z)], w.at[pl.ds(0, Z - 1), 0, pl.ds(0, 64)]),
        ]
        own = [
            Ring(lambda k, h: [w.at[k, x, pl.ds(h * 32, 32)]], w.at[0, 0, pl.ds(0, 32)], z, Z, at_z),
            Ring(lambda k, h: [w.at[z, k, pl.ds(64 + h * 32, 32)]], w.at[0, 0, pl.ds(0, 32)], x, X, at_x),
        ]
        most = w.at[0, pl.ds(0, X - 1), pl.ds(0, 32)]
        rest = [
            Ring(lambda k, h: others(lambda n: w.at[k, n, pl.ds(0, 64)], x, X, h), most, z, Z, at_z),
            Ring(lambda k, h: others(lambda n: w.at[n, k, pl.ds(64, 64)], z, Z, h), most, x, X, at_x),
        ]
        return first, own, rest

    def short_gather_of(w):
        def send(f, blocks, at, size, whole):
            pairs = [(ref, ref, at(d)) for k in blocks for ref in [half_block(w, f, k)] for d in range(1, size)]
            return group_of(ids(1), pairs, whole)

        def half_block(w, f, k):
            at_zx = (z, (x + k) % X) if f == 0 else ((z + k) % Z, x)
            return w.at[at_zx[0], at_zx[1], pl.ds(64 * f, 64)]

        few, many = w.at[0, pl.ds(0, X - 1), pl.ds(0, 64)], w.at[pl.ds(0, Z - 1), pl.ds(0, X - 1), pl.ds(0, 64)]
        first = [send(0, [0], at_x, X, few), send(1, [0], at_z, Z, few)]
        own = [send(0, [0], at_z, Z, few), send(1, [0], at_x, X, few)]
        rest = [send(0, range(1, X), at_z, Z, many), send(1, range(1, Z), at_x, X, many)]
        return first, own, rest

    first_a, own_a, rest_a = short_gather_of(w_a)
    first_b, own_b, rest_b = gather_of(w_b)
    own_gain = gain_all.at[slot]
    gains = group_of(ids(1), [(own_gain, own_gain, at_tp(d)) for d in range(1, TP)], gain_all.at[pl.ds(0, TP - 1)], 1)
    tile_0, tile_1 = o_w.at[c, 0, z, x, own_rows], o_w.at[c, 1, z, x, own_rows]
    out_0 = [
        group_of(ids(1), [(tile_0, tile_0, at_x(d)) for d in range(1, X)], fsend.at[0, pl.ds(0, (X - 1) * 128)]),
        group_of(ids(1), [(tile_1, tile_1, at_z(d)) for d in range(1, Z)], fsend.at[0, pl.ds(0, (Z - 1) * 128)]),
    ]
    def rows_from(k):
        return pl.ds(pl.multiple_of(k * 128, 128), 128)

    quarter = o_w.at[0, 0, 0, pl.ds(0, half_x), pl.ds(0, 128)]
    out_1 = [
        Ring(lambda k, h: [o_w.at[c, 0, z, pl.ds(h * half_x, half_x), rows_from(k)]], quarter, y, Y, at_y),
        Ring(lambda k, h: [o_w.at[c, 1, pl.ds(h * half_z, half_z), x, rows_from(k)]], quarter, y, Y, at_y),
    ]
    out_2 = [
        Ring(lambda k, h: [o_w.at[c, 0, k, pl.ds(h * half_x, half_x)]], o_w.at[0, 0, 0, pl.ds(0, half_x)], z, Z, at_z),
        Ring(lambda k, h: [o_w.at[c, 1, pl.ds(h * half_z, half_z), k]], o_w.at[0, 0, 0, pl.ds(0, half_x)], x, X, at_x),
    ]

    def to_partner(d):
        row, column = o_w.at[c, 0, (z + d) % Z], o_w.at[c, 1, :, (x + d) % X]
        return [(row, row, partner), (column, column, partner)]

    pair_1 = group_of(ids(1), to_partner(0), o_w.at[0, 0, pl.ds(0, 2)])
    pairs = [pair_1]
    if X == 2:
        pair_4 = group_of(ids(1), to_partner(1), o_w.at[0, 0, pl.ds(0, 2)])
        pairs += [pair_4]
    else:
        passed = [(ref, ref, partner) for ring in out_2 for ref in ring.passed]
        rest = [(ref, ref, partner) for ring in out_2 for ref in ring.rest]
        pair_2 = group_of(ids(1), passed, o_w.at[0, 0, pl.ds(0, 2)])
        pair_3 = group_of(ids(1), rest, o_w.at[0, 0, pl.ds(0, 2)])
        pair_4 = group_of(ids(1), to_partner(2), o_w.at[0, 0, pl.ds(0, 2)])
        pairs += [pair_2, pair_3, pair_4]

    rim_i, keys_i = ids(SEQS), ids(SEQS)

    def rims(s):
        return group_of(
            rim_i + s,
            [
                (gpad.at[s, pl.ds(RIM, RIM)], gpad.at[s, pl.ds(RIM + T, RIM)], left),
                (gpad.at[s, pl.ds(T, RIM)], gpad.at[s, pl.ds(0, RIM)], right),
            ],
            gpad.at[0, pl.ds(0, 2 * RIM)],
        )

    def edge_keys(s):
        return group_of(
            keys_i + s,
            [(edges.at[s, 1], edges.at[s, 3], left), (edges.at[s, 2], edges.at[s, 0], right)],
            edges.at[0, pl.ds(0, 2)],
        )

    conv_i, attn_i = ids(SEQS), ids(SEQS)
    peers_rows = fsend.at[0, pl.ds(0, (TP - 1) * 128)]

    def rows_of(device_tp):
        return pl.ds(pl.multiple_of(device_tp * 128, 128), 128)

    conv_lanes = pl.ds(pl.multiple_of(slot * 128, 128), 128)
    attn_lanes = pl.ds(pl.multiple_of(c * (Y * 256) + (Y + y) * 128, 128), 128)

    def conv_out_copies(s):
        return group_of(
            conv_i + s,
            [
                (fsend.at[s, rows_of((tp + d) % TP)], cbm.at[s, :, conv_lanes], at_tp(d))
                for d in range(1, TP)
            ],
            peers_rows,
        )

    def attn_out_copies(s):
        return group_of(
            attn_i + s,
            [
                (asend.at[s, rows_of((tp + d) % TP)], bm.at[s, :, attn_lanes], at_tp(d))
                for d in range(1, TP)
            ],
            peers_rows,
        )

    for n in range(2):
        loads[n].wait()
    with jax.named_scope("greet"):
        pl.semaphore_wait(barrier, len(greeted))
    for group in first_a + own_a:
        start(group[0])

    for n in (8, 9, 10):
        loads[n].wait()
    run = turn_buf.shape[1] - NSP - 32
    cos_s, sin_s = turn_buf[0, pl.ds(run + 32 + sp, 1), :], turn_buf[1, pl.ds(run + 32 + sp, 1), :]
    cos_b, sin_b = turn_buf[0, run : run + 32, :], turn_buf[1, run : run + 32, :]
    cos_bs, sin_bs = cos_b * cos_s - sin_b * sin_s, sin_b * cos_s + cos_b * sin_s
    low_half = (lax.broadcasted_iota(jnp.int32, (1, 128), 1) % HEAD_DIM) < HEAD_DIM // 2
    sign = jnp.where(low_half, -1.0, 1.0)

    def turn(n, carry):
        cos_a, sin_a = turn_buf[0, pl.ds(n, 1), :], turn_buf[1, pl.ds(n, 1), :]
        at = pl.ds(pl.multiple_of(n * 32, 32), 32)
        cos_ref[at, :] = cos_bs * cos_a - sin_bs * sin_a
        sin_ref[at, :] = (sin_bs * cos_a + cos_bs * sin_a) * sign
        return carry

    lax.fori_loop(0, T // 32, turn, 0, unroll=2)

    for n in (5, 6, 7):
        loads[n].wait()
    loads[2].wait()
    w_b[z, x, :, 0:128] = (w_b[z, x, :, 0:128].astype(F32) * HEAD_DIM**-0.5).astype(BF16)
    w_b[z, x, :, 128:256] = key_buf[...].astype(F32).T.astype(BF16)
    taps_buf[...] = taps_rows[...].astype(F32)
    for n in range(D // 128):
        gain_buf[:, n * 128 : (n + 1) * 128] = jnp.broadcast_to(
            gain_rows[n : n + 1, :].astype(F32), (16, 128)
        )
    loads[11].wait()
    gain_all[slot] = jnp.broadcast_to(conv_gain_row[...].astype(F32), (8, 128))
    key_i = lax.broadcasted_iota(jnp.int32, (WINDOW, 256), 0)
    query_i = lax.broadcasted_iota(jnp.int32, (WINDOW, 256), 1) % WINDOW
    bias[0] = jnp.where(key_i >= query_i, 0.0, MASK_VALUE)
    bias[1] = jnp.where(key_i <= query_i, 0.0, MASK_VALUE)
    for n in range(3, 5):
        loads[n].wait()

    def ln_block(i, carry):
        tok_copy(i).wait()

        @pl.when(i + SLOTS - 1 < n_blocks)
        def _():
            tok_copy(i + SLOTS - 1).start()

        def group(g, carry):
            at = pl.ds(pl.multiple_of(i * LN_ROWS, LN_ROWS) + pl.multiple_of(g * 16, 16), 16)
            v = tbuf[i % SLOTS, pl.ds(pl.multiple_of(g * 16, 16), 16), :].astype(F32)
            mean = jnp.sum(v, axis=-1, keepdims=True) * (1.0 / D)
            centred = v - mean
            var = jnp.sum(centred * centred, axis=-1, keepdims=True) * (1.0 / D)
            out = centred * lax.rsqrt(var + EPSILON) * gain_buf[...]
            normed[at, :] = out.astype(BF16)
            return carry

        return lax.fori_loop(0, LN_ROWS // 16, group, carry, unroll=16)

    def norm_blocks(first, last):
        with jax.named_scope("norm"):
            lax.fori_loop(n_blocks * first // 16, n_blocks * last // 16, ln_block, 0)

    norm_blocks(0, 2)
    for group in first_b + out_0 + [gains]:
        start(group[0])
    norm_blocks(2, 5)
    with jax.named_scope("wait_in_1"):
        for group in first_a:
            arrived(group)
    for group in rest_a:
        start(group[0])
    for ring in own_b:
        ring.begin()
    norm_blocks(5, 9)
    with jax.named_scope("wait_in_b1"):
        for group in first_b:
            arrived(group)
    for ring in rest_b:
        ring.begin()
    norm_blocks(9, 11)
    with jax.named_scope("wait_out_0"):
        for group in out_0:
            arrived(group)
    for ring in out_1:
        ring.begin_direct()
    for ring in out_1:
        ring.begin_late()
    norm_blocks(11, 16)
    with jax.named_scope("wait_in_a"):
        for group in own_a + rest_a:
            arrived(group)

    lane = lax.broadcasted_iota(jnp.int32, (1, 128), 1)
    low_head = lane < HEAD_DIM

    def swapped(v):
        return jnp.where(low_half, pltpu.roll(v, 96, 1), pltpu.roll(v, 32, 1))

    def gate(s, starts):
        n = 256 // len(starts)
        at = [pl.ds(pl.multiple_of(s * T + r, 128), n) for r in starts]
        rows = jnp.concatenate([normed[rs, :] for rs in at], axis=0)
        a = dot(rows, w_a[...].reshape(D, 256))
        gated = a[:, :128] * jax.nn.sigmoid(a[:, 128:])
        gated = gated.astype(BF16).astype(F32)
        for k in range(2):
            r = pl.multiple_of(starts[k] if len(starts) == 2 else starts[0] + k * 128, 128)
            gpad[s, pl.ds(RIM + r, 128), :] = gated[k * 128 : (k + 1) * 128]

    def project(s, starts):
        n = 256 // len(starts)
        at = [pl.ds(pl.multiple_of(s * T + r, 128), n) for r in starts]
        rows = jnp.concatenate([normed[rs, :] for rs in at], axis=0)
        b = dot(rows, w_b[...].reshape(D, 256))
        at = [pl.ds(pl.multiple_of(r, 128), n) for r in starts]
        cosine = jnp.concatenate([cos_ref[rs, :] for rs in at], axis=0)
        sine = jnp.concatenate([sin_ref[rs, :] for rs in at], axis=0)
        q, kv = b[:, :128], b[:, 128:]
        q = q * cosine + swapped(q) * sine
        zero = jnp.zeros_like(q)
        q_0 = jnp.where(low_head, q, zero).astype(BF16)
        q_1 = jnp.where(low_head, zero, q).astype(BF16)
        turned = kv * cosine + swapped(kv) * sine
        twice = jnp.where(low_head, turned, pltpu.roll(turned, 64, 1)).astype(BF16)
        kv = jnp.where(low_head, turned, kv).astype(BF16)
        for k in range(2):
            r = pl.multiple_of(starts[k] if len(starts) == 2 else starts[0] + k * 128, 128)
            part = slice(k * 128, (k + 1) * 128)
            qz[s, r // 128, 0] = q_0[part]
            qz[s, r // 128, 1] = q_1[part]
            kpad[s, pl.ds(WINDOW + r, 128), :] = twice[part]
            val_t[s, :, pl.ds(WINDOW + r, 128)] = kv[part].T[64:]
            if len(starts) == 2:
                edges[s, k + 1] = kv[part]

    def convolve(s):
        with jax.named_scope("wait_rim"):
            arrived(rims(s))

        @pl.when(sp == 0)
        def _():
            gpad[s, pl.ds(0, RIM), :] = jnp.zeros((RIM, 128), F32)

        @pl.when(sp == NSP - 1)
        def _():
            gpad[s, pl.ds(RIM + T, RIM), :] = jnp.zeros((RIM, 128), F32)

        def chunk(k, carry):
            r = pl.multiple_of(k * 128, 128)
            total = jnp.zeros((128, 128), F32)
            for j in range(31):
                total = total + gpad[s, pl.ds(r + (j + 1), 128), :] * taps_buf[pl.ds(j, 1), :]
            fsend[s, pl.ds(r, 128), :] = total.astype(BF16)
            return carry

        with jax.named_scope("conv"):
            lax.fori_loop(0, T // 128, chunk, 0)
        start(conv_out_copies(s)[0])
        cbm[s, :, conv_lanes] = fsend[s, rows_of(tp), :]

    def gate_edges(k, carry):
        for s in (2 * k, 2 * k + 1):
            gate(s, (0, T - 128))
        for s in (2 * k, 2 * k + 1):
            start(rims(s)[0])
        return carry

    def project_edges(k, carry):
        for s in (2 * k, 2 * k + 1):
            project(s, (0, T - 128))
        for s in (2 * k, 2 * k + 1):
            start(edge_keys(s)[0])
        return carry

    inner = T // 256 - 1

    def inner_rows(s, step):
        lax.fori_loop(0, inner, lambda k, carry: step(s, (128 + k * 256,)) or carry, 0, unroll=inner)

    def gate_inner(s, carry):
        inner_rows(s, gate)
        return carry

    def each_convolve(s, carry):
        convolve(s)
        return carry

    with jax.named_scope("gate_edges"):
        lax.fori_loop(0, SEQS // 2, gate_edges, 0)
    with jax.named_scope("wait_relay_b"):
        for ring in own_b + rest_b + out_1:
            ring.relay()
    with jax.named_scope("gate_inner"):
        lax.fori_loop(0, SEQS, gate_inner, 0)
    with jax.named_scope("wait_out_1"):
        for ring in out_1:
            ring.near()
            ring.finish()
    for ring in out_2:
        ring.begin_direct()
    lax.fori_loop(0, SEQS // 2, each_convolve, 0)
    with jax.named_scope("wait_in_b"):
        for ring in own_b + rest_b:
            ring.near()
            ring.finish()
    with jax.named_scope("project_edges"):
        lax.fori_loop(0, SEQS // 2, project_edges, 0)
    for ring in out_2:
        ring.begin_late()
    start(pair_1[0])
    lax.fori_loop(SEQS // 2, SEQS, each_convolve, 0)

    head_lane = lax.broadcasted_iota(jnp.int32, (1, 256), 1)
    sink_row = jnp.where(head_lane < 128, sink[0], sink[1])

    def widen(s, e, first):
        kv = edges[s, e].astype(F32)
        kpad[s, pl.ds(first, WINDOW), :] = jnp.where(low_head, kv, pltpu.roll(kv, 64, 1)).astype(BF16)
        val_t[s, :, pl.ds(first, WINDOW)] = edges[s, e].T[64:]

    blocks = T // 128

    def attend(s):
        with jax.named_scope("wait_keys"):
            arrived(edge_keys(s))
        widen(s, 0, 0)
        widen(s, 3, WINDOW + T)

        tops, totals = {}, {}

        def score(b):
            keys = kpad[s, pl.ds(b * 128, 384), :]
            scores = dot(keys, qz[s, b].reshape(256, 128), ((1,), (1,)))
            low, high = bias[0], bias[1]
            if b == 0:
                low = low + jnp.where(sp == 0, MASK_VALUE, 0.0)
            if b == blocks - 1:
                high = high + jnp.where(sp == NSP - 1, MASK_VALUE, 0.0)
            s_0, s_1, s_2 = scores[:128] + low, scores[128:256], scores[256:] + high
            top = jnp.max(jnp.maximum(jnp.maximum(s_0, s_1), s_2), axis=0, keepdims=True)
            tops[b] = jnp.maximum(top, sink_row)
            for n, part in enumerate((s_0, s_1, s_2)):
                score_buf[b % 2, n] = part

        def weigh(b):
            top = tops[b]
            e_0, e_1, e_2 = (jnp.exp(score_buf[b % 2, n] - top) for n in range(3))
            total = jnp.sum(e_0 + e_1 + e_2, axis=0, keepdims=True) + jnp.exp(sink_row - top)
            totals[b] = total
            logs = top + jnp.log(total)
            log_total[s, :, pl.ds(b * 128, 128)] = jnp.concatenate([logs[:, :128], logs[:, 128:]], axis=0)
            for n, part in enumerate((e_0, e_1, e_2)):
                weight_buf[b % 2, n] = part.astype(BF16)

        def collect(b):
            weights = weight_buf[b % 2].reshape(384, 256)
            out = dot(val_t[s, :, pl.ds(b * 128, 384)], weights) * (1.0 / totals[b])
            both = jnp.concatenate([out[:, :128], out[:, 128:]], axis=0)
            asend[s, pl.ds(b * 128, 128), :] = both.astype(BF16).T

        with jax.named_scope("attend"):
            for b in range(blocks + 2):
                if b < blocks:
                    score(b)
                if 0 <= b - 1 < blocks:
                    weigh(b - 1)
                if b >= 2:
                    collect(b - 2)
        @pl.when(s == SEQS - 1)
        def _():
            with jax.named_scope("wait_out_2"):
                for ring in out_2:
                    ring.finish()
            start(pair_4[0])

        start(attn_out_copies(s)[0])
        bm[s, :, attn_lanes] = asend[s, rows_of(tp), :]

    def sequence(s, carry):
        with jax.named_scope("project"):
            inner_rows(s, project)

        @pl.when(s == SEQS - 2)
        def _():
            with jax.named_scope("wait_out_near"):
                for ring in out_2:
                    ring.near()
            if X > 2:
                start(pair_3[0])

        @pl.when(s == 0)
        def _():
            with jax.named_scope("wait_out_relay"):
                for ring in out_2:
                    ring.relay()
            if X > 2:
                start(pair_2[0])

        attend(s)
        return carry

    lax.fori_loop(0, SEQS, sequence, 0)
    arrived(gains)

    def finish(s):
        with jax.named_scope("wait_conv"):
            arrived(conv_out_copies(s))

        def group(g, carry):
            at = pl.ds(pl.multiple_of(g * 16, 16), 16)
            v = cbm[s, at, :].astype(F32)
            mean = jnp.sum(v, axis=-1, keepdims=True) * (1.0 / (TP * 128))
            centred = v - mean
            var = jnp.sum(centred * centred, axis=-1, keepdims=True) * (1.0 / (TP * 128))
            scale = lax.rsqrt(var + EPSILON)
            for n in range(TP):
                u = centred[:, n * 128 : (n + 1) * 128] * scale * gain_all[n, 0:1, :]
                first = n // Y * (Y * 256) + n % Y * 128
                bm[s, at, first : first + 128] = jax.nn.silu(u).astype(BF16)
            return carry

        with jax.named_scope("channel_norm"):
            lax.fori_loop(0, 128 // 16, group, 0, unroll=8)

    def out_pair(blocks, h):
        at = [((z + dz) % Z, (x + dx) % X) for dz, dx in blocks]
        pieces = [
            jnp.concatenate([o_w[cc, hh, zz, xx] for zz, xx in at], axis=1)
            for cc in range(CORES)
            for hh in h
        ]
        columns = [pl.ds(pl.multiple_of((zz * X + xx) * 128, 128), 128) for zz, xx in at]
        return jnp.concatenate(pieces, axis=0), columns

    everything = [(dz, dx) for dz in range(Z) for dx in range(X)]
    early = [k for k in everything if X > 2 and 2 not in k]
    early = early[: len(early) // 2 * 2]
    late = [k for k in everything if k not in early]
    early, late = ([b[n : n + 2] for n in range(0, len(b), 2)] for b in (early, late))
    branch = Y * 128
    half = SEQS // 2

    def rows_out(seqs, h):
        first = [(2 * cc + h) * branch for cc in range(CORES)]
        n = seqs.stop - seqs.start
        lanes = [bm[seqs, :, k : k + branch].reshape(n * 128, branch) for k in first]
        return jnp.concatenate(lanes, axis=1)

    def out_conv(n, blocks):
        acc = dot(rows_out(slice(0, SEQS), 0), out_pair(blocks, (0,))[0])
        partial_out[n] = acc.reshape(SEQS, 128, 256)

    def out_attn(n, blocks, seqs):
        weights, columns = out_pair(blocks, (1,))
        count = seqs.stop - seqs.start
        acc = dot(rows_out(seqs, 1), weights).reshape(count, 128, 256) + partial_out[n, seqs]
        acc = acc.astype(BF16)
        for n in range(2):
            mixed[seqs, :, columns[n]] = acc[:, :, n * 128 : (n + 1) * 128]

    early = list(enumerate(early))
    late = [(len(early) + n, blocks) for n, blocks in enumerate(late)]
    for s in range(SEQS):
        finish(s)
    with jax.named_scope("wait_pair"):
        for group in pairs[:-1]:
            arrived(group)
    with jax.named_scope("out_conv"):
        for n, blocks in early:
            out_conv(n, blocks)
    with jax.named_scope("wait_attn"):
        for s in range(half):
            arrived(attn_out_copies(s))
    with jax.named_scope("out_attn"):
        for n, blocks in early:
            out_attn(n, blocks, slice(0, half))
    with jax.named_scope("wait_pair"):
        arrived(pair_4)
    with jax.named_scope("out_conv"):
        for n, blocks in late:
            out_conv(n, blocks)
    with jax.named_scope("out_attn"):
        for n, blocks in late:
            out_attn(n, blocks, slice(0, half))
    with jax.named_scope("wait_attn"):
        for s in range(half, SEQS):
            arrived(attn_out_copies(s))
    with jax.named_scope("out_attn"):
        for n, blocks in early + late:
            out_attn(n, blocks, slice(half, SEQS))

    rings = own_b + rest_b + out_1 + out_2
    groups = first_a + own_a + rest_a + first_b + out_0 + pairs + [group for ring in rings for group in ring.groups()]
    for s in range(SEQS):
        groups += [rims(s), edge_keys(s), conv_out_copies(s), attn_out_copies(s)]
    sent_rows = sum(group[2] for group in groups) // (2 * D)
    gains[1].wait_send()
    while sent_rows > 0:
        gone = normed.at[pl.ds(0, min(sent_rows, SEQS * T))]
        remote(gone, gone, 0, right).wait_send()
        sent_rows -= SEQS * T


def on_device(
    grid_shape,
    tokens,
    norm_gain,
    conv_value_weight,
    conv_gate_weight,
    query_weight,
    key_weight,
    value_weight,
    conv_taps,
    conv_gain,
    sink_logit,
    out_conv_weight,
    out_attn_weight,
):
    seqs, toks, width = tokens.shape
    xs, zs, ys, tps = grid_shape
    n_sp = xs * zs
    half = HEAD_DIM // 2
    inverse = (ROPE_BASE ** (-np.arange(half, dtype=np.float32) / half)).astype(np.float32)
    parts = [np.arange(toks // 32) * 32, np.arange(32), np.arange(n_sp) * toks]
    angles = np.concatenate(parts)[:, None] * np.tile(inverse.astype(np.float64), 4)[None, :]
    turns = np.stack([np.cos(angles), np.sin(angles)]).astype(np.float32)

    n_copies = 6 + 26 + 2 + 12 + 1 + 12 + 4 + 4 * seqs
    vmem = pl.BlockSpec(memory_space=pltpu.VMEM)
    far = pl.BlockSpec(memory_space=pl.ANY)
    call = pl.pallas_call(
        functools.partial(kernel, (seqs, toks, width, xs, zs, ys, tps)),
        out_shape=(
            pltpu.VMEM((seqs, toks // tps, width), BF16),
            pltpu.VMEM((seqs, 2, toks), F32),
        ),
        in_specs=[far] * 9 + [pl.BlockSpec(memory_space=pltpu.SMEM)] + [far] * 3,
        out_specs=(vmem, vmem),
        scratch_shapes=[
            pltpu.VMEM((SLOTS, LN_ROWS, width), BF16),
            pltpu.VMEM((16, width), F32),
            pltpu.VMEM((seqs * toks, width), BF16),
            pltpu.VMEM((zs, xs, 128, 256), BF16),
            pltpu.VMEM((zs, xs, 128, 256), BF16),
            pltpu.VMEM((CORES, 2, zs, xs, ys * 128, 128), BF16),
            pltpu.VMEM((tps, 8, 128), F32),
            pltpu.VMEM((31, 128), F32),
            pltpu.VMEM((128, 128), BF16),
            pltpu.VMEM((width // 128, 128), BF16),
            pltpu.VMEM((31, 128), BF16),
            pltpu.VMEM((1, 128), BF16),
            pltpu.VMEM(turns.shape, F32),
            pltpu.VMEM((toks, 128), F32),
            pltpu.VMEM((toks, 128), F32),
            pltpu.VMEM((seqs, toks + 2 * RIM, 128), F32),
            pltpu.VMEM((seqs, toks // 128, 2, 128, 128), BF16),
            pltpu.VMEM((seqs, toks + 2 * WINDOW, 128), BF16),
            pltpu.VMEM((seqs, HEAD_DIM, toks + 2 * WINDOW), BF16),
            pltpu.VMEM((seqs, 4, WINDOW, 128), BF16),
            pltpu.VMEM((2, WINDOW, 256), F32),
            pltpu.VMEM((2, 3, WINDOW, 256), F32),
            pltpu.VMEM((2, 3, WINDOW, 256), BF16),
            pltpu.VMEM((xs * zs // 2, seqs, 128, 256), F32),
            pltpu.VMEM((seqs, toks, 128), BF16),
            pltpu.VMEM((seqs, toks, 128), BF16),
            pltpu.VMEM((seqs, toks // tps, tps * 128), BF16),
            pltpu.VMEM((seqs, toks // tps, tps * 256), BF16),
            pltpu.SemaphoreType.DMA((SLOTS,)),
            pltpu.SemaphoreType.DMA((12,)),
            pltpu.SemaphoreType.DMA((2,)),
            pltpu.SemaphoreType.DMA((n_copies,)),
        ],
        compiler_params=pltpu.CompilerParams(
            collective_id=0, has_side_effects=True, vmem_limit_bytes=54 * 2**20
        ),
        name="layer",
    )
    return call(
        tokens,
        norm_gain.reshape(-1, 128),
        conv_value_weight,
        conv_gate_weight,
        query_weight,
        key_weight.T,
        value_weight.T,
        conv_taps,
        conv_gain.reshape(1, -1),
        sink_logit,
        out_conv_weight,
        out_attn_weight,
        jnp.asarray(turns),
    )


def solution(mesh):
    placed = (
        P(None, "sp", None),
        P(),
        P("sp", "tp"),
        P("sp", "tp"),
        P("sp", "tp"),
        P("sp", "tp"),
        P("sp", "tp"),
        P(None, "tp"),
        P("tp"),
        P("tp"),
        P("tp", "sp"),
        P("tp", "sp"),
    )
    xs = int(round(mesh.shape["sp"] ** 0.5))
    shape = (xs, mesh.shape["sp"] // xs, mesh.shape["tp"] // CORES, mesh.shape["tp"])
    return jax.shard_map(
        functools.partial(on_device, shape),
        mesh=mesh,
        in_specs=placed,
        out_specs=(P(None, ("sp", "tp"), None), P(None, "tp", "sp")),
        check_vma=False,
    )
```

```python
import functools
import math

import jax
import jax.numpy as jnp
import numpy as np
from jax import lax
from jax.experimental import pallas as pl
from jax.experimental.pallas import tpu as pltpu
from jax.sharding import PartitionSpec as P

MESH = pl.DeviceIdType.MESH
F32 = jnp.float32
BF16 = jnp.bfloat16

HEAD_DIM = 64
WINDOW = 128
EPSILON = 1e-06
ROPE_BASE = 10000.0
MASK_VALUE = -1e30
RIM = 16
LN_ROWS = 256
CORES = 2
SLOTS = 6


def dot(a, b, dims=((1,), (0,))):
    return lax.dot_general(a, b, (dims, ((), ())), preferred_element_type=F32)


def kernel(
    dims,
    tokens,
    norm_gain,
    w_value,
    w_gate,
    w_query,
    w_key,
    w_val,
    conv_taps,
    conv_gain,
    sink,
    w_oc,
    w_oa,
    turns,
    mixed,
    log_total,
    tbuf,
    gain_buf,
    normed,
    w_a,
    w_b,
    o_w,
    gain_all,
    taps_buf,
    key_buf,
    gain_rows,
    taps_rows,
    conv_gain_row,
    turn_buf,
    cos_ref,
    sin_ref,
    gpad,
    qz,
    kpad,
    val_t,
    edges,
    bias,
    score_buf,
    weight_buf,
    partial_out,
    fsend,
    asend,
    cbm,
    bm,
    tok_sem,
    load_sem,
    send_sem,
    recv_sem,
):
    SEQS, T, D, X, Z, Y, TP = dims
    NSP = X * Z
    per_seq = T // LN_ROWS
    n_blocks = SEQS * per_seq
    sp, tp = lax.axis_index("sp"), lax.axis_index("tp")
    z, x = sp // X, sp % X
    y, c = tp // CORES, tp % CORES
    slot = c * Y + y
    own_rows = pl.ds(pl.multiple_of(y * 128, 128), 128)

    def at_x(d):
        return (z * X + (x + d) % X, tp)

    def at_z(d):
        return (((z + d) % Z) * X + x, tp)

    def at_y(d):
        return (sp, ((y + d) % Y) * CORES + c)

    def at_tp(d):
        return (sp, (tp + d) % TP)

    partner = (sp, y * CORES + (1 - c))
    right = ((sp + 1) % NSP, tp)
    left = ((sp + NSP - 1) % NSP, tp)

    counter = [0]

    def ids(n):
        first = counter[0]
        counter[0] += n
        return first

    def remote(src, dst, i, device, sent=0):
        return pltpu.make_async_remote_copy(
            src_ref=src,
            dst_ref=dst,
            send_sem=send_sem.at[sent],
            recv_sem=recv_sem.at[i],
            device_id=device,
            device_id_type=MESH,
        )

    def start(copies):
        for cp in copies:
            cp.start()

    def group_of(i, pairs, whole, sent=0):
        copies = [remote(src, dst, i, device, sent) for src, dst, device in pairs]
        return copies, remote(whole, whole, i, right, sent), math.prod(whole.shape) * whole.dtype.itemsize

    def arrived(group):
        group[1].wait_recv()

    class Ring:
        def __init__(self, part, whole, me, size, at):
            i = ids(6)
            before, after = (me + size - 1) % size, (me + 1) % size

            def half(n, k, h, d):
                return group_of(i + n, [(ref, ref, at(d)) for ref in part(k, h)], whole)

            self.direct = [half(0, me, 0, 1)]
            self.relayed, self.late = [], [half(1, me, 1, 1)]
            self.passed, self.rest = [], []
            if size == 2:
                return
            self.direct.append(half(2, me, 1, size - 1))
            self.late.append(half(3, me, 0, size - 1))
            self.relayed = [half(4, before, 0, 1), half(5, after, 1, size - 1)]
            self.passed = part(before, 0) + part(after, 1)
            self.rest = part(before, 1) + part(after, 0)

        def begin(self):
            self.begin_direct()
            self.begin_late()

        def begin_direct(self):
            for group in self.direct:
                start(group[0])

        def begin_late(self):
            for group in self.late:
                start(group[0])

        def relay(self):
            for group in self.direct:
                arrived(group)
            for group in self.relayed:
                start(group[0])

        def near(self):
            for group in self.late:
                arrived(group)

        def finish(self):
            for group in self.relayed:
                arrived(group)

        def groups(self):
            return self.direct + self.late + self.relayed

    def tok_copy(i):
        seq, r = i // per_seq, (i % per_seq) * LN_ROWS
        return pltpu.make_async_copy(
            tokens.at[seq, pl.ds(pl.multiple_of(r, LN_ROWS), LN_ROWS)],
            tbuf.at[i % SLOTS],
            tok_sem.at[i % SLOTS],
        )

    barrier = pltpu.get_barrier_semaphore()
    greeted = (
        [at_x(d) for d in range(1, X)]
        + [at_z(d) for d in range(1, Z)]
        + [left, right]
        + [at_tp(d) for d in range(1, TP)]
    )
    for device in greeted:
        pl.semaphore_signal(barrier, inc=1, device_id=device, device_id_type=MESH)

    wanted = [
        (w_value, w_a.at[z, x, :, pl.ds(0, 128)]),
        (w_gate, w_a.at[z, x, :, pl.ds(128, 128)]),
        (w_query, w_b.at[z, x, :, pl.ds(0, 128)]),
        (w_oc, o_w.at[c, 0, z, x, own_rows]),
        (w_oa, o_w.at[c, 1, z, x, own_rows]),
        (w_key, key_buf.at[pl.ds(0, 64)]),
        (w_val, key_buf.at[pl.ds(64, 64)]),
        (conv_taps, taps_rows),
        (turns.at[0], turn_buf.at[0]),
        (turns.at[1], turn_buf.at[1]),
        (norm_gain, gain_rows),
        (conv_gain, conv_gain_row),
    ]
    loads = [pltpu.make_async_copy(a, b, load_sem.at[n]) for n, (a, b) in enumerate(wanted)]
    for n in (5, 6, 8, 9, 0, 1, 2, 3, 4, 7, 10, 11):
        loads[n].start()

    for n in range(SLOTS - 1):
        tok_copy(n).start()

    half_x, half_z = X // 2, Z // 2

    def others(block, me, size, h):
        if size == 2:
            return [block(1 - me).at[pl.ds(h * 32, 32)]]
        opposite = block((me + 2) % size).at[pl.ds(h * 32, 32)]
        return [block((me + 1 + 2 * h) % size), opposite]

    def gather_of(w):
        mine = [w.at[z, x, pl.ds(64 * f, 64)] for f in range(2)]
        first = [
            group_of(ids(1), [(mine[0], mine[0], at_x(d)) for d in range(1, X)], w.at[0, pl.ds(0, X - 1), pl.ds(0, 64)]),
            group_of(ids(1), [(mine[1], mine[1], at_z(d)) for d in range(1, Z)], w.at[pl.ds(0, Z - 1), 0, pl.ds(0, 64)]),
        ]
        own = [
            Ring(lambda k, h: [w.at[k, x, pl.ds(h * 32, 32)]], w.at[0, 0, pl.ds(0, 32)], z, Z, at_z),
            Ring(lambda k, h: [w.at[z, k, pl.ds(64 + h * 32, 32)]], w.at[0, 0, pl.ds(0, 32)], x, X, at_x),
        ]
        most = w.at[0, pl.ds(0, X - 1), pl.ds(0, 32)]
        rest = [
            Ring(lambda k, h: others(lambda n: w.at[k, n, pl.ds(0, 64)], x, X, h), most, z, Z, at_z),
            Ring(lambda k, h: others(lambda n: w.at[n, k, pl.ds(64, 64)], z, Z, h), most, x, X, at_x),
        ]
        return first, own, rest

    def short_gather_of(w):
        def send(f, blocks, at, size, whole):
            pairs = [(ref, ref, at(d)) for k in blocks for ref in [half_block(w, f, k)] for d in range(1, size)]
            return group_of(ids(1), pairs, whole)

        def half_block(w, f, k):
            at_zx = (z, (x + k) % X) if f == 0 else ((z + k) % Z, x)
            return w.at[at_zx[0], at_zx[1], pl.ds(64 * f, 64)]

        few, many = w.at[0, pl.ds(0, X - 1), pl.ds(0, 64)], w.at[pl.ds(0, Z - 1), pl.ds(0, X - 1), pl.ds(0, 64)]
        first = [send(0, [0], at_x, X, few), send(1, [0], at_z, Z, few)]
        own = [send(0, [0], at_z, Z, few), send(1, [0], at_x, X, few)]
        rest = [send(0, range(1, X), at_z, Z, many), send(1, range(1, Z), at_x, X, many)]
        return first, own, rest

    first_a, own_a, rest_a = short_gather_of(w_a)
    first_b, own_b, rest_b = gather_of(w_b)
    own_gain = gain_all.at[slot]
    gains = group_of(ids(1), [(own_gain, own_gain, at_tp(d)) for d in range(1, TP)], gain_all.at[pl.ds(0, TP - 1)], 1)
    tile_0, tile_1 = o_w.at[c, 0, z, x, own_rows], o_w.at[c, 1, z, x, own_rows]
    out_0 = [
        group_of(ids(1), [(tile_0, tile_0, at_x(d)) for d in range(1, X)], fsend.at[0, pl.ds(0, (X - 1) * 128)]),
        group_of(ids(1), [(tile_1, tile_1, at_z(d)) for d in range(1, Z)], fsend.at[0, pl.ds(0, (Z - 1) * 128)]),
    ]
    def rows_from(k):
        return pl.ds(pl.multiple_of(k * 128, 128), 128)

    quarter = o_w.at[0, 0, 0, pl.ds(0, half_x), pl.ds(0, 128)]
    out_1 = [
        Ring(lambda k, h: [o_w.at[c, 0, z, pl.ds(h * half_x, half_x), rows_from(k)]], quarter, y, Y, at_y),
        Ring(lambda k, h: [o_w.at[c, 1, pl.ds(h * half_z, half_z), x, rows_from(k)]], quarter, y, Y, at_y),
    ]
    out_2 = [
        Ring(lambda k, h: [o_w.at[c, 0, k, pl.ds(h * half_x, half_x)]], o_w.at[0, 0, 0, pl.ds(0, half_x)], z, Z, at_z),
        Ring(lambda k, h: [o_w.at[c, 1, pl.ds(h * half_z, half_z), k]], o_w.at[0, 0, 0, pl.ds(0, half_x)], x, X, at_x),
    ]

    def to_partner(d):
        row, column = o_w.at[c, 0, (z + d) % Z], o_w.at[c, 1, :, (x + d) % X]
        return [(row, row, partner), (column, column, partner)]

    pair_1 = group_of(ids(1), to_partner(0), o_w.at[0, 0, pl.ds(0, 2)])
    pairs = [pair_1]
    if X == 2:
        pair_4 = group_of(ids(1), to_partner(1), o_w.at[0, 0, pl.ds(0, 2)])
        pairs += [pair_4]
    else:
        passed = [(ref, ref, partner) for ring in out_2 for ref in ring.passed]
        rest = [(ref, ref, partner) for ring in out_2 for ref in ring.rest]
        pair_2 = group_of(ids(1), passed, o_w.at[0, 0, pl.ds(0, 2)])
        pair_3 = group_of(ids(1), rest, o_w.at[0, 0, pl.ds(0, 2)])
        pair_4 = group_of(ids(1), to_partner(2), o_w.at[0, 0, pl.ds(0, 2)])
        pairs += [pair_2, pair_3, pair_4]

    rim_i, keys_i = ids(SEQS), ids(SEQS)

    def rims(s):
        return group_of(
            rim_i + s,
            [
                (gpad.at[s, pl.ds(RIM, RIM)], gpad.at[s, pl.ds(RIM + T, RIM)], left),
                (gpad.at[s, pl.ds(T, RIM)], gpad.at[s, pl.ds(0, RIM)], right),
            ],
            gpad.at[0, pl.ds(0, 2 * RIM)],
        )

    def edge_keys(s):
        return group_of(
            keys_i + s,
            [(edges.at[s, 1], edges.at[s, 3], left), (edges.at[s, 2], edges.at[s, 0], right)],
            edges.at[0, pl.ds(0, 2)],
        )

    conv_i, attn_i = ids(SEQS), ids(SEQS)
    peers_rows = fsend.at[0, pl.ds(0, (TP - 1) * 128)]

    def rows_of(device_tp):
        return pl.ds(pl.multiple_of(device_tp * 128, 128), 128)

    conv_lanes = pl.ds(pl.multiple_of(slot * 128, 128), 128)
    attn_lanes = pl.ds(pl.multiple_of(c * (Y * 256) + (Y + y) * 128, 128), 128)

    def conv_out_copies(s):
        return group_of(
            conv_i + s,
            [
                (fsend.at[s, rows_of((tp + d) % TP)], cbm.at[s, :, conv_lanes], at_tp(d))
                for d in range(1, TP)
            ],
            peers_rows,
        )

    def attn_out_copies(s):
        return group_of(
            attn_i + s,
            [
                (asend.at[s, rows_of((tp + d) % TP)], bm.at[s, :, attn_lanes], at_tp(d))
                for d in range(1, TP)
            ],
            peers_rows,
        )

    for n in range(2):
        loads[n].wait()
    with jax.named_scope("greet"):
        pl.semaphore_wait(barrier, len(greeted))
    for group in first_a + own_a:
        start(group[0])

    for n in (8, 9, 10):
        loads[n].wait()
    run = turn_buf.shape[1] - NSP - 32
    cos_s, sin_s = turn_buf[0, pl.ds(run + 32 + sp, 1), :], turn_buf[1, pl.ds(run + 32 + sp, 1), :]
    cos_b, sin_b = turn_buf[0, run : run + 32, :], turn_buf[1, run : run + 32, :]
    cos_bs, sin_bs = cos_b * cos_s - sin_b * sin_s, sin_b * cos_s + cos_b * sin_s
    low_half = (lax.broadcasted_iota(jnp.int32, (1, 128), 1) % HEAD_DIM) < HEAD_DIM // 2
    sign = jnp.where(low_half, -1.0, 1.0)

    def turn(n, carry):
        cos_a, sin_a = turn_buf[0, pl.ds(n, 1), :], turn_buf[1, pl.ds(n, 1), :]
        at = pl.ds(pl.multiple_of(n * 32, 32), 32)
        cos_ref[at, :] = cos_bs * cos_a - sin_bs * sin_a
        sin_ref[at, :] = (sin_bs * cos_a + cos_bs * sin_a) * sign
        return carry

    lax.fori_loop(0, T // 32, turn, 0, unroll=2)

    for n in (5, 6, 7):
        loads[n].wait()
    loads[2].wait()
    w_b[z, x, :, 0:128] = (w_b[z, x, :, 0:128].astype(F32) * HEAD_DIM**-0.5).astype(BF16)
    w_b[z, x, :, 128:256] = key_buf[...].astype(F32).T.astype(BF16)
    taps_buf[...] = taps_rows[...].astype(F32)
    for n in range(D // 128):
        gain_buf[:, n * 128 : (n + 1) * 128] = jnp.broadcast_to(
            gain_rows[n : n + 1, :].astype(F32), (16, 128)
        )
    loads[11].wait()
    gain_all[slot] = jnp.broadcast_to(conv_gain_row[...].astype(F32), (8, 128))
    key_i = lax.broadcasted_iota(jnp.int32, (WINDOW, 256), 0)
    query_i = lax.broadcasted_iota(jnp.int32, (WINDOW, 256), 1) % WINDOW
    bias[0] = jnp.where(key_i >= query_i, 0.0, MASK_VALUE)
    bias[1] = jnp.where(key_i <= query_i, 0.0, MASK_VALUE)
    for n in range(3, 5):
        loads[n].wait()

    def ln_block(i, carry):
        tok_copy(i).wait()

        @pl.when(i + SLOTS - 1 < n_blocks)
        def _():
            tok_copy(i + SLOTS - 1).start()

        def group(g, carry):
            at = pl.ds(pl.multiple_of(i * LN_ROWS, LN_ROWS) + pl.multiple_of(g * 16, 16), 16)
            v = tbuf[i % SLOTS, pl.ds(pl.multiple_of(g * 16, 16), 16), :].astype(F32)
            mean = jnp.sum(v, axis=-1, keepdims=True) * (1.0 / D)
            centred = v - mean
            var = jnp.sum(centred * centred, axis=-1, keepdims=True) * (1.0 / D)
            out = centred * lax.rsqrt(var + EPSILON) * gain_buf[...]
            normed[at, :] = out.astype(BF16)
            return carry

        return lax.fori_loop(0, LN_ROWS // 16, group, carry, unroll=16)

    def norm_blocks(first, last):
        with jax.named_scope("norm"):
            lax.fori_loop(n_blocks * first // 16, n_blocks * last // 16, ln_block, 0)

    norm_blocks(0, 2)
    for group in first_b + out_0 + [gains]:
        start(group[0])
    norm_blocks(2, 5)
    with jax.named_scope("wait_in_1"):
        for group in first_a:
            arrived(group)
    for group in rest_a:
        start(group[0])
    for ring in own_b:
        ring.begin()
    norm_blocks(5, 9)
    with jax.named_scope("wait_in_b1"):
        for group in first_b:
            arrived(group)
    for ring in rest_b:
        ring.begin()
    norm_blocks(9, 11)
    with jax.named_scope("wait_out_0"):
        for group in out_0:
            arrived(group)
    for ring in out_1:
        ring.begin_direct()
    for ring in out_1:
        ring.begin_late()
    norm_blocks(11, 16)
    with jax.named_scope("wait_in_a"):
        for group in own_a + rest_a:
            arrived(group)

    lane = lax.broadcasted_iota(jnp.int32, (1, 128), 1)
    low_head = lane < HEAD_DIM

    def swapped(v):
        return jnp.where(low_half, pltpu.roll(v, 96, 1), pltpu.roll(v, 32, 1))

    def gate(s, starts):
        n = 256 // len(starts)
        at = [pl.ds(pl.multiple_of(s * T + r, 128), n) for r in starts]
        rows = jnp.concatenate([normed[rs, :] for rs in at], axis=0)
        a = dot(rows, w_a[...].reshape(D, 256))
        gated = a[:, :128] * jax.nn.sigmoid(a[:, 128:])
        gated = gated.astype(BF16).astype(F32)
        for k in range(2):
            r = pl.multiple_of(starts[k] if len(starts) == 2 else starts[0] + k * 128, 128)
            gpad[s, pl.ds(RIM + r, 128), :] = gated[k * 128 : (k + 1) * 128]

    def project(s, starts):
        n = 256 // len(starts)
        at = [pl.ds(pl.multiple_of(s * T + r, 128), n) for r in starts]
        rows = jnp.concatenate([normed[rs, :] for rs in at], axis=0)
        b = dot(rows, w_b[...].reshape(D, 256))
        at = [pl.ds(pl.multiple_of(r, 128), n) for r in starts]
        cosine = jnp.concatenate([cos_ref[rs, :] for rs in at], axis=0)
        sine = jnp.concatenate([sin_ref[rs, :] for rs in at], axis=0)
        q, kv = b[:, :128], b[:, 128:]
        q = q * cosine + swapped(q) * sine
        zero = jnp.zeros_like(q)
        q_0 = jnp.where(low_head, q, zero).astype(BF16)
        q_1 = jnp.where(low_head, zero, q).astype(BF16)
        turned = kv * cosine + swapped(kv) * sine
        twice = jnp.where(low_head, turned, pltpu.roll(turned, 64, 1)).astype(BF16)
        kv = jnp.where(low_head, turned, kv).astype(BF16)
        for k in range(2):
            r = pl.multiple_of(starts[k] if len(starts) == 2 else starts[0] + k * 128, 128)
            part = slice(k * 128, (k + 1) * 128)
            qz[s, r // 128, 0] = q_0[part]
            qz[s, r // 128, 1] = q_1[part]
            kpad[s, pl.ds(WINDOW + r, 128), :] = twice[part]
            val_t[s, :, pl.ds(WINDOW + r, 128)] = kv[part].T[64:]
            if len(starts) == 2:
                edges[s, k + 1] = kv[part]

    def convolve(s):
        with jax.named_scope("wait_rim"):
            arrived(rims(s))

        @pl.when(sp == 0)
        def _():
            gpad[s, pl.ds(0, RIM), :] = jnp.zeros((RIM, 128), F32)

        @pl.when(sp == NSP - 1)
        def _():
            gpad[s, pl.ds(RIM + T, RIM), :] = jnp.zeros((RIM, 128), F32)

        def chunk(k, carry):
            r = pl.multiple_of(k * 128, 128)
            total = jnp.zeros((128, 128), F32)
            for j in range(31):
                total = total + gpad[s, pl.ds(r + (j + 1), 128), :] * taps_buf[pl.ds(j, 1), :]
            fsend[s, pl.ds(r, 128), :] = total.astype(BF16)
            return carry

        with jax.named_scope("conv"):
            lax.fori_loop(0, T // 128, chunk, 0)
        start(conv_out_copies(s)[0])
        cbm[s, :, conv_lanes] = fsend[s, rows_of(tp), :]

    def gate_edges(k, carry):
        for s in (2 * k, 2 * k + 1):
            gate(s, (0, T - 128))
        for s in (2 * k, 2 * k + 1):
            start(rims(s)[0])
        return carry

    def project_edges(k, carry):
        for s in (2 * k, 2 * k + 1):
            project(s, (0, T - 128))
        for s in (2 * k, 2 * k + 1):
            start(edge_keys(s)[0])
        return carry

    inner = T // 256 - 1

    def inner_rows(s, step):
        lax.fori_loop(0, inner, lambda k, carry: step(s, (128 + k * 256,)) or carry, 0, unroll=inner)

    def gate_inner(s, carry):
        inner_rows(s, gate)
        return carry

    def each_convolve(s, carry):
        convolve(s)
        return carry

    with jax.named_scope("gate_edges"):
        lax.fori_loop(0, SEQS // 2, gate_edges, 0)
    with jax.named_scope("wait_relay_b"):
        for ring in own_b + rest_b + out_1:
            ring.relay()
    with jax.named_scope("gate_inner"):
        lax.fori_loop(0, SEQS, gate_inner, 0)
    with jax.named_scope("wait_out_1"):
        for ring in out_1:
            ring.near()
            ring.finish()
    for ring in out_2:
        ring.begin_direct()
    lax.fori_loop(0, SEQS // 2, each_convolve, 0)
    with jax.named_scope("wait_in_b"):
        for ring in own_b + rest_b:
            ring.near()
            ring.finish()
    with jax.named_scope("project_edges"):
        lax.fori_loop(0, SEQS // 2, project_edges, 0)
    for ring in out_2:
        ring.begin_late()
    start(pair_1[0])
    lax.fori_loop(SEQS // 2, SEQS, each_convolve, 0)

    head_lane = lax.broadcasted_iota(jnp.int32, (1, 256), 1)
    sink_row = jnp.where(head_lane < 128, sink[0], sink[1])

    def widen(s, e, first):
        kv = edges[s, e].astype(F32)
        kpad[s, pl.ds(first, WINDOW), :] = jnp.where(low_head, kv, pltpu.roll(kv, 64, 1)).astype(BF16)
        val_t[s, :, pl.ds(first, WINDOW)] = edges[s, e].T[64:]

    blocks = T // 128

    def attend(s):
        with jax.named_scope("wait_keys"):
            arrived(edge_keys(s))
        widen(s, 0, 0)
        widen(s, 3, WINDOW + T)

        tops, totals = {}, {}

        def score(b):
            keys = kpad[s, pl.ds(b * 128, 384), :]
            scores = dot(keys, qz[s, b].reshape(256, 128), ((1,), (1,)))
            low, high = bias[0], bias[1]
            if b == 0:
                low = low + jnp.where(sp == 0, MASK_VALUE, 0.0)
            if b == blocks - 1:
                high = high + jnp.where(sp == NSP - 1, MASK_VALUE, 0.0)
            s_0, s_1, s_2 = scores[:128] + low, scores[128:256], scores[256:] + high
            top = jnp.max(jnp.maximum(jnp.maximum(s_0, s_1), s_2), axis=0, keepdims=True)
            tops[b] = jnp.maximum(top, sink_row)
            for n, part in enumerate((s_0, s_1, s_2)):
                score_buf[b % 2, n] = part

        def weigh(b):
            top = tops[b]
            e_0, e_1, e_2 = (jnp.exp(score_buf[b % 2, n] - top) for n in range(3))
            total = jnp.sum(e_0 + e_1 + e_2, axis=0, keepdims=True) + jnp.exp(sink_row - top)
            totals[b] = total
            logs = top + jnp.log(total)
            log_total[s, :, pl.ds(b * 128, 128)] = jnp.concatenate([logs[:, :128], logs[:, 128:]], axis=0)
            for n, part in enumerate((e_0, e_1, e_2)):
                weight_buf[b % 2, n] = part.astype(BF16)

        def collect(b):
            weights = weight_buf[b % 2].reshape(384, 256)
            out = dot(val_t[s, :, pl.ds(b * 128, 384)], weights) * (1.0 / totals[b])
            both = jnp.concatenate([out[:, :128], out[:, 128:]], axis=0)
            asend[s, pl.ds(b * 128, 128), :] = both.astype(BF16).T

        with jax.named_scope("attend"):
            for b in range(blocks + 2):
                if b < blocks:
                    score(b)
                if 0 <= b - 1 < blocks:
                    weigh(b - 1)
                if b >= 2:
                    collect(b - 2)
        @pl.when(s == SEQS - 1)
        def _():
            with jax.named_scope("wait_out_2"):
                for ring in out_2:
                    ring.finish()
            start(pair_4[0])

        start(attn_out_copies(s)[0])
        bm[s, :, attn_lanes] = asend[s, rows_of(tp), :]

    def sequence(s, carry):
        with jax.named_scope("project"):
            inner_rows(s, project)

        @pl.when(s == SEQS - 2)
        def _():
            with jax.named_scope("wait_out_near"):
                for ring in out_2:
                    ring.near()
            if X > 2:
                start(pair_3[0])

        @pl.when(s == 0)
        def _():
            with jax.named_scope("wait_out_relay"):
                for ring in out_2:
                    ring.relay()
            if X > 2:
                start(pair_2[0])

        attend(s)
        return carry

    lax.fori_loop(0, SEQS, sequence, 0)
    arrived(gains)

    def finish(s):
        with jax.named_scope("wait_conv"):
            arrived(conv_out_copies(s))

        def group(g, carry):
            at = pl.ds(pl.multiple_of(g * 16, 16), 16)
            v = cbm[s, at, :].astype(F32)
            mean = jnp.sum(v, axis=-1, keepdims=True) * (1.0 / (TP * 128))
            centred = v - mean
            var = jnp.sum(centred * centred, axis=-1, keepdims=True) * (1.0 / (TP * 128))
            scale = lax.rsqrt(var + EPSILON)
            for n in range(TP):
                u = centred[:, n * 128 : (n + 1) * 128] * scale * gain_all[n, 0:1, :]
                first = n // Y * (Y * 256) + n % Y * 128
                bm[s, at, first : first + 128] = jax.nn.silu(u).astype(BF16)
            return carry

        with jax.named_scope("channel_norm"):
            lax.fori_loop(0, 128 // 16, group, 0, unroll=8)

    def out_pair(blocks, h):
        at = [((z + dz) % Z, (x + dx) % X) for dz, dx in blocks]
        pieces = [
            jnp.concatenate([o_w[cc, hh, zz, xx] for zz, xx in at], axis=1)
            for cc in range(CORES)
            for hh in h
        ]
        columns = [pl.ds(pl.multiple_of((zz * X + xx) * 128, 128), 128) for zz, xx in at]
        return jnp.concatenate(pieces, axis=0), columns

    everything = [(dz, dx) for dz in range(Z) for dx in range(X)]
    early = [k for k in everything if X > 2 and 2 not in k]
    early = early[: len(early) // 2 * 2]
    late = [k for k in everything if k not in early]
    early, late = ([b[n : n + 2] for n in range(0, len(b), 2)] for b in (early, late))
    branch = Y * 128
    half = SEQS // 2

    def rows_out(seqs, h):
        first = [(2 * cc + h) * branch for cc in range(CORES)]
        n = seqs.stop - seqs.start
        lanes = [bm[seqs, :, k : k + branch].reshape(n * 128, branch) for k in first]
        return jnp.concatenate(lanes, axis=1)

    def out_conv(n, blocks):
        acc = dot(rows_out(slice(0, SEQS), 0), out_pair(blocks, (0,))[0])
        partial_out[n] = acc.reshape(SEQS, 128, 256)

    def out_attn(n, blocks, seqs):
        weights, columns = out_pair(blocks, (1,))
        count = seqs.stop - seqs.start
        acc = dot(rows_out(seqs, 1), weights).reshape(count, 128, 256) + partial_out[n, seqs]
        acc = acc.astype(BF16)
        for n in range(2):
            mixed[seqs, :, columns[n]] = acc[:, :, n * 128 : (n + 1) * 128]

    early = list(enumerate(early))
    late = [(len(early) + n, blocks) for n, blocks in enumerate(late)]
    for s in range(SEQS):
        finish(s)
    with jax.named_scope("wait_pair"):
        for group in pairs[:-1]:
            arrived(group)
    with jax.named_scope("out_conv"):
        for n, blocks in early:
            out_conv(n, blocks)
    with jax.named_scope("wait_attn"):
        for s in range(half):
            arrived(attn_out_copies(s))
    with jax.named_scope("out_attn"):
        for n, blocks in early:
            out_attn(n, blocks, slice(0, half))
    with jax.named_scope("wait_pair"):
        arrived(pair_4)
    with jax.named_scope("out_conv"):
        for n, blocks in late:
            out_conv(n, blocks)
    with jax.named_scope("out_attn"):
        for n, blocks in late:
            out_attn(n, blocks, slice(0, half))
    with jax.named_scope("wait_attn"):
        for s in range(half, SEQS):
            arrived(attn_out_copies(s))
    with jax.named_scope("out_attn"):
        for n, blocks in early + late:
            out_attn(n, blocks, slice(half, SEQS))

    rings = own_b + rest_b + out_1 + out_2
    groups = first_a + own_a + rest_a + first_b + out_0 + pairs + [group for ring in rings for group in ring.groups()]
    for s in range(SEQS):
        groups += [rims(s), edge_keys(s), conv_out_copies(s), attn_out_copies(s)]
    sent_rows = sum(group[2] for group in groups) // (2 * D)
    gains[1].wait_send()
    while sent_rows > 0:
        gone = normed.at[pl.ds(0, min(sent_rows, SEQS * T))]
        remote(gone, gone, 0, right).wait_send()
        sent_rows -= SEQS * T


def put(mixed, log_total, mixed_out, log_out, sem):
    seqs = mixed.shape[0]
    copies = [pltpu.make_async_copy(log_total, log_out, sem.at[seqs])]
    copies += [pltpu.make_async_copy(mixed.at[s], mixed_out.at[s], sem.at[s]) for s in range(seqs)]
    for cp in copies:
        cp.start()
    for cp in copies:
        cp.wait()


def on_device(
    grid_shape,
    tokens,
    norm_gain,
    conv_value_weight,
    conv_gate_weight,
    query_weight,
    key_weight,
    value_weight,
    conv_taps,
    conv_gain,
    sink_logit,
    out_conv_weight,
    out_attn_weight,
):
    seqs, toks, width = tokens.shape
    xs, zs, ys, tps = grid_shape
    n_sp = xs * zs
    half = HEAD_DIM // 2
    inverse = (ROPE_BASE ** (-np.arange(half, dtype=np.float32) / half)).astype(np.float32)
    parts = [np.arange(toks // 32) * 32, np.arange(32), np.arange(n_sp) * toks]
    angles = np.concatenate(parts)[:, None] * np.tile(inverse.astype(np.float64), 4)[None, :]
    turns = np.stack([np.cos(angles), np.sin(angles)]).astype(np.float32)

    n_copies = 6 + 26 + 2 + 12 + 1 + 12 + 4 + 4 * seqs
    vmem = pl.BlockSpec(memory_space=pltpu.VMEM)
    far = pl.BlockSpec(memory_space=pl.ANY)
    call = pl.pallas_call(
        functools.partial(kernel, (seqs, toks, width, xs, zs, ys, tps)),
        out_shape=(
            pltpu.VMEM((seqs, toks // tps, width), BF16),
            pltpu.VMEM((seqs, 2, toks), F32),
        ),
        in_specs=[far] * 9 + [pl.BlockSpec(memory_space=pltpu.SMEM)] + [far] * 3,
        out_specs=(vmem, vmem),
        scratch_shapes=[
            pltpu.VMEM((SLOTS, LN_ROWS, width), BF16),
            pltpu.VMEM((16, width), F32),
            pltpu.VMEM((seqs * toks, width), BF16),
            pltpu.VMEM((zs, xs, 128, 256), BF16),
            pltpu.VMEM((zs, xs, 128, 256), BF16),
            pltpu.VMEM((CORES, 2, zs, xs, ys * 128, 128), BF16),
            pltpu.VMEM((tps, 8, 128), F32),
            pltpu.VMEM((31, 128), F32),
            pltpu.VMEM((128, 128), BF16),
            pltpu.VMEM((width // 128, 128), BF16),
            pltpu.VMEM((31, 128), BF16),
            pltpu.VMEM((1, 128), BF16),
            pltpu.VMEM(turns.shape, F32),
            pltpu.VMEM((toks, 128), F32),
            pltpu.VMEM((toks, 128), F32),
            pltpu.VMEM((seqs, toks + 2 * RIM, 128), F32),
            pltpu.VMEM((seqs, toks // 128, 2, 128, 128), BF16),
            pltpu.VMEM((seqs, toks + 2 * WINDOW, 128), BF16),
            pltpu.VMEM((seqs, HEAD_DIM, toks + 2 * WINDOW), BF16),
            pltpu.VMEM((seqs, 4, WINDOW, 128), BF16),
            pltpu.VMEM((2, WINDOW, 256), F32),
            pltpu.VMEM((2, 3, WINDOW, 256), F32),
            pltpu.VMEM((2, 3, WINDOW, 256), BF16),
            pltpu.VMEM((xs * zs // 2, seqs, 128, 256), F32),
            pltpu.VMEM((seqs, toks, 128), BF16),
            pltpu.VMEM((seqs, toks, 128), BF16),
            pltpu.VMEM((seqs, toks // tps, tps * 128), BF16),
            pltpu.VMEM((seqs, toks // tps, tps * 256), BF16),
            pltpu.SemaphoreType.DMA((SLOTS,)),
            pltpu.SemaphoreType.DMA((12,)),
            pltpu.SemaphoreType.DMA((2,)),
            pltpu.SemaphoreType.DMA((n_copies,)),
        ],
        compiler_params=pltpu.CompilerParams(
            collective_id=0, has_side_effects=True, vmem_limit_bytes=54 * 2**20
        ),
        name="layer",
    )
    mixed, log_total = call(
        tokens,
        norm_gain.reshape(-1, 128),
        conv_value_weight,
        conv_gate_weight,
        query_weight,
        key_weight.T,
        value_weight.T,
        conv_taps,
        conv_gain.reshape(1, -1),
        sink_logit,
        out_conv_weight,
        out_attn_weight,
        jnp.asarray(turns),
    )
    return pl.pallas_call(
        put,
        out_shape=(jax.ShapeDtypeStruct(mixed.shape, BF16), jax.ShapeDtypeStruct(log_total.shape, F32)),
        in_specs=[far, far],
        out_specs=(far, far),
        scratch_shapes=[pltpu.SemaphoreType.DMA((seqs + 1,))],
        compiler_params=pltpu.CompilerParams(vmem_limit_bytes=2**20),
        name="put",
    )(mixed, log_total)


def solution(mesh):
    placed = (
        P(None, "sp", None),
        P(),
        P("sp", "tp"),
        P("sp", "tp"),
        P("sp", "tp"),
        P("sp", "tp"),
        P("sp", "tp"),
        P(None, "tp"),
        P("tp"),
        P("tp"),
        P("tp", "sp"),
        P("tp", "sp"),
    )
    xs = int(round(mesh.shape["sp"] ** 0.5))
    shape = (xs, mesh.shape["sp"] // xs, mesh.shape["tp"] // CORES, mesh.shape["tp"])
    return jax.shard_map(
        functools.partial(on_device, shape),
        mesh=mesh,
        in_specs=placed,
        out_specs=(P(None, ("sp", "tp"), None), P(None, "tp", "sp")),
        check_vma=False,
    )
```
